512 devices in a mesh: sp: 32 (over z, core), tp: 16 (over y, x).
Axes of the slice: x: 4, y: 4, z: 16, core: 2. Of those that a mesh axis runs over, the one named last changes fastest.
Arguments:
- moe_in: bfloat16 [6144, 2048], P('sp'), may hold values from -6 to 6
- cotangent: bfloat16 [6144, 2048], P('sp'), may hold values from -6 to 6
- routing: int32 [6144, 2], P('sp'), may hold values from 0 to 31, as said below
- route_weight: float32 [6144, 2], P('sp'), may hold values from 0.2 to 1
- w_gate: bfloat16 [32, 2048, 2048], P('sp', 'tp'), may hold values from -0.125 to 0.125
- w_up: bfloat16 [32, 2048, 2048], P('sp', 'tp'), may hold values from -0.125 to 0.125
- w_down: bfloat16 [32, 2048, 2048], P('sp', 'tp'), may hold values from -0.125 to 0.125
- gate_b: bfloat16 [1024, 6144], P('tp', 'sp'), may hold values from -6 to 6
- gate_c: bfloat16 [1024, 6144], P('tp', 'sp'), may hold values from -6 to 6
- value_x: bfloat16 [1024, 6144], P('tp', 'sp'), may hold values from -6 to 6
- conv_taps: float32 [3, 1024], P(None, 'tp'), may hold values from -3 to 3
- out_proj: bfloat16 [1024, 2048], P('tp'), may hold values from -0.1875 to 0.1875
Outputs:
- w_gate_grad: bfloat16 [32, 2048, 2048], P('sp', 'tp')
- w_up_grad: bfloat16 [32, 2048, 2048], P('sp', 'tp')
- w_down_grad: bfloat16 [32, 2048, 2048], P('sp', 'tp')
- moe_in_grad: bfloat16 [6144, 2048], P('sp', 'tp')
- proj_grad: float32 [1024, 2048], P('tp', 'sp')
- gate_b_grad: bfloat16 [1024, 6144], P('tp', 'sp')
- gate_c_grad: bfloat16 [1024, 6144], P('tp', 'sp')
- value_x_grad: bfloat16 [1024, 6144], P('tp', 'sp')
The draws below stay inside these ranges and needn't reach their ends.
Inputs may be any that keep to these rules, and one draw needn't show every extreme that they name: `routing`: in each aligned block of 192 rows every expert is named exactly 12 times. The two entries of a row are different experts of one group; group g holds experts g * 8 to g * 8 + 7.
All inputs are finite; a program needn't handle non-finite values.
Results may differ from the reference program's by a relative error of at most 0.025.
Values may be sent and summed in bfloat16 or wider, within the bound.
A program may use at most 64 MiB of HBM per device.

```python
import jax
import jax.numpy as jnp
from jax import lax

D = 2048
W_A = 1024
HID = 2048
TAPS = 3
GROUPS = 4
TOPK = 2
TOK_DEV = 192
TOKENS = 6144
EXPERTS = 32
CAP = 12
HID_DEV = 128
N_SP = 32
N_TP = 16


def route_block(block_key):
    per_group = EXPERTS // GROUPS
    key_rank, key_shift, key_group, key_local = jax.random.split(block_key, 4)
    rank = jax.random.permutation(key_rank, TOK_DEV).astype(jnp.int32)
    first = rank % EXPERTS
    cycle = rank // EXPERTS
    offset = jax.random.randint(key_shift, (), 0, per_group, dtype=jnp.int32)
    shift = (cycle + offset) % max(per_group - 1, 1)
    group_id = first // per_group
    local_one = first % per_group
    local_two = (local_one + 1 + shift) % per_group
    group_perm = jax.random.permutation(key_group, GROUPS).astype(jnp.int32)
    local_perm = jax.random.permutation(key_local, per_group).astype(jnp.int32)
    expert_one = group_perm[group_id] * per_group + local_perm[local_one]
    expert_two = group_perm[group_id] * per_group + local_perm[local_two]
    return jnp.stack([expert_one, expert_two], axis=1)


def draw_routing(key, part):
    block_keys = jax.random.split(jax.random.fold_in(key, 17), TOKENS // TOK_DEV)
    blocks = jax.vmap(route_block)(block_keys)
    return blocks.reshape(TOKENS, TOPK).astype(jnp.int32)


def with_spikes(array, key, source, target, shards_of, factor):
    owner, partner = [(jnp.arange(array.shape[axis_at]) // (array.shape[axis_at] // shards_of)).reshape([-1 if axis == axis_at else 1 for axis in range(array.ndim)]) for axis_at in (source, target)]
    chosen = jax.random.permutation(key, shards_of)[partner]
    strong = (owner == chosen) | (owner == (partner + shards_of // 2) % shards_of)
    return jnp.where(strong, factor * array, array)


def block_scale(stream_key, shape, shards, smallest, top_value):
    loudness = 1.0
    for position, parts in shards:
        heights = jax.random.uniform(jax.random.fold_in(jax.random.fold_in(stream_key, 6), position), (parts,), jnp.float32, smallest / len(shards), top_value / len(shards))
        loudness = loudness * jnp.repeat(jnp.exp(heights), shape[position] // parts).reshape((-1,) + (1,) * (len(shape) - 1 - position))
    return loudness


def gaussian(stream_key, extent, scale, bound, cuts=(), kind=jnp.bfloat16):
    entries = scale * jax.random.normal(stream_key, extent, jnp.float32)
    if cuts:
        entries = entries * block_scale(stream_key, extent, cuts, -0.22, 0.18)
    return jnp.clip(entries, -bound, bound).astype(kind)


def gaussian_with(key, dims, deviation, most, cuts, heavy, kind=jnp.bfloat16):
    result = deviation * jax.random.normal(key, dims, jnp.float32)
    if cuts:
        result = result * block_scale(key, dims, cuts, -0.22, 0.18)
    return jnp.clip(with_spikes(result, jax.random.fold_in(key, 3), *heavy), -most, most).astype(kind)


def setup_inputs(seed: int = 0) -> dict:
    key_list = jax.random.split(jax.random.key(seed), 13)
    return {
        "moe_in": gaussian(key_list[0], (TOKENS, D), 1.0, 6.0, ((0, 32),)),
        "cotangent": gaussian_with(key_list[1], (TOKENS, D), 1.0, 6.0, ((0, 32),), (0, 1, 32, 2.75)),
        "routing": draw_routing(jax.random.fold_in(key_list[12], 71), 0),
        "route_weight": jnp.clip(0.2 + 0.8 * jax.random.uniform(key_list[3], (TOKENS, TOPK), jnp.float32) ** block_scale(key_list[3], (TOKENS, TOPK), ((0, 32),), -0.2, 0.2), 0.2, 1.0),
        "w_gate": gaussian(key_list[4], (EXPERTS, HID, D), D ** -0.5, 0.125, ((0, 32), (1, 16))),
        "w_up": gaussian(key_list[5], (EXPERTS, HID, D), D ** -0.5, 0.125, ((0, 32), (1, 16))),
        "w_down": gaussian(key_list[6], (EXPERTS, HID, D), HID ** -0.5, 0.125, ((0, 32), (1, 16))),
        "gate_b": gaussian(key_list[7], (W_A, TOKENS), 1.0, 6.0, ((0, 16), (1, 32))),
        "gate_c": gaussian(key_list[8], (W_A, TOKENS), 1.0, 6.0, ((0, 16), (1, 32))),
        "value_x": gaussian(key_list[9], (W_A, TOKENS), 1.0, 6.0, ((0, 16), (1, 32))),
        "conv_taps": gaussian(key_list[10], (TAPS, W_A), 0.6, 3.0, ((1, 16),), jnp.float32),
        "out_proj": gaussian(key_list[11], (W_A, D), W_A ** -0.5, 0.1875, ((0, 16),)),
    }


def reference(moe_in, cotangent, routing, route_weight, w_gate, w_up, w_down, gate_b, gate_c, value_x, conv_taps, out_proj):
    flat_routes = routing.reshape(-1)
    order = jnp.argsort(flat_routes, stable=True).astype(jnp.int32).reshape(EXPERTS, CAP * N_SP)
    weight_flat = route_weight.reshape(-1)
    contract_model = (((1,), (1,)), ((), ()))
    over_rows = (((0,), (0,)), ((), ()))

    def expert(packed):
        index, gate_weight, up_weight, down_weight = packed
        owner = index // TOPK
        arrived = moe_in[owner]
        route_cot = (weight_flat[index][:, None] * cotangent[owner].astype(jnp.float32)).astype(jnp.bfloat16)
        gate_pre = lax.dot_general(arrived, gate_weight, contract_model, preferred_element_type=jnp.float32)
        up_pre = lax.dot_general(arrived, up_weight, contract_model, preferred_element_type=jnp.float32)
        sigmoid_gate = jax.nn.sigmoid(gate_pre)
        hidden = (gate_pre * sigmoid_gate * up_pre).astype(jnp.bfloat16)
        hidden_grad = lax.dot_general(route_cot, down_weight, contract_model, preferred_element_type=jnp.float32)
        gate_grad = (hidden_grad * up_pre * sigmoid_gate * (1.0 + gate_pre * (1.0 - sigmoid_gate))).astype(jnp.bfloat16)
        up_grad = (hidden_grad * gate_pre * sigmoid_gate).astype(jnp.bfloat16)
        gate_wgrad = lax.dot_general(gate_grad, arrived, over_rows, preferred_element_type=jnp.float32).astype(jnp.bfloat16)
        up_wgrad = lax.dot_general(up_grad, arrived, over_rows, preferred_element_type=jnp.float32).astype(jnp.bfloat16)
        down_wgrad = lax.dot_general(hidden, route_cot, over_rows, preferred_element_type=jnp.float32).astype(jnp.bfloat16)
        row_total = gate_grad.shape[0]
        gate_blocks = gate_grad.astype(jnp.float32).reshape(row_total, N_TP, HID_DEV)
        up_blocks = up_grad.astype(jnp.float32).reshape(row_total, N_TP, HID_DEV)
        gate_table = gate_weight.astype(jnp.float32).reshape(N_TP, HID_DEV, D)
        up_table = up_weight.astype(jnp.float32).reshape(N_TP, HID_DEV, D)
        partial_value = jnp.einsum("rbh,bhd->brd", gate_blocks, gate_table) + jnp.einsum("rbh,bhd->brd", up_blocks, up_table)
        partial_value = lax.optimization_barrier(partial_value.astype(jnp.bfloat16)).astype(jnp.float32)
        route_grad = jnp.sum(partial_value, axis=0).astype(jnp.bfloat16)
        return gate_wgrad, up_wgrad, down_wgrad, route_grad

    w_gate_grad, w_up_grad, w_down_grad, route_grads = lax.map(expert, (order, w_gate, w_up, w_down))
    placed = jnp.zeros((TOKENS * TOPK, D), jnp.float32).at[order.reshape(-1)].set(route_grads.reshape(-1, D).astype(jnp.float32))
    moe_in_grad = jnp.sum(placed.reshape(TOKENS, TOPK, D), axis=1).astype(jnp.bfloat16)

    stream_grad = (cotangent.astype(jnp.float32) + moe_in_grad.astype(jnp.float32)).astype(jnp.bfloat16)
    mixed_in = lax.optimization_barrier((gate_c.astype(jnp.float32) * value_x.astype(jnp.float32)).astype(jnp.bfloat16))
    extended = jnp.pad(mixed_in.astype(jnp.float32), ((0, 0), (TAPS - 1, 0)))
    conv_out = jnp.zeros((W_A, TOKENS), jnp.float32)
    for tap in range(TAPS):
        conv_out = conv_out + conv_taps[tap][:, None] * extended[:, tap:tap + TOKENS]
    mixer_act = (gate_b.astype(jnp.float32) * conv_out).astype(jnp.bfloat16)
    act_grad = lax.dot_general(out_proj, stream_grad, contract_model, preferred_element_type=jnp.float32)
    proj_grad = jnp.dot(mixer_act, stream_grad, preferred_element_type=jnp.float32)
    gate_b_grad = (act_grad * conv_out).astype(jnp.bfloat16)
    conv_grad = act_grad * gate_b.astype(jnp.float32)
    extended_grad = jnp.pad(conv_grad, ((0, 0), (0, TAPS - 1)))
    mixed_grad = jnp.zeros((W_A, TOKENS), jnp.float32)
    for tap in range(TAPS):
        offset = TAPS - 1 - tap
        mixed_grad = mixed_grad + conv_taps[tap][:, None] * extended_grad[:, offset:offset + TOKENS]
    gate_c_grad = (mixed_grad * value_x.astype(jnp.float32)).astype(jnp.bfloat16)
    value_x_grad = (mixed_grad * gate_c.astype(jnp.float32)).astype(jnp.bfloat16)
    return (w_gate_grad, w_up_grad, w_down_grad, moe_in_grad, proj_grad, gate_b_grad, gate_c_grad, value_x_grad)
```

```python
import functools

import jax
import jax.numpy as jnp
from jax import lax
from jax.experimental import pallas as pl
from jax.experimental.pallas import tpu as pltpu
from jax.sharding import PartitionSpec as P

MESH = pl.DeviceIdType.MESH
BF = jnp.bfloat16
F32 = jnp.float32
VM = pltpu.VMEM

OFFSETS = (0, 1, -2, 3, -4, 5, -6, 7, -1, 2, -3, 4, -5, 6, -7, 8)
PLACE = {d % 16: j for j, d in enumerate(OFFSETS)}
SLOT = 16
CAP = 12


def nt(a, b):
    return lax.dot_general(a, b, (((1,), (1,)), ((), ())), preferred_element_type=F32)


def nn(a, b):
    return jnp.dot(a, b, preferred_element_type=F32)


def tn(a, b):
    return lax.dot_general(a, b, (((0,), (0,)), ((), ())), preferred_element_type=F32)


def kernel(
    moe_h, cot_h, route_t, weight, wg_h, wu_h, wd_h, gb_h, gc_h, vx_h, taps, op_h,
    o_wg, o_wu, o_wd, o_moe, o_proj, o_gb, o_gc, o_vx,
    moe_v, cot_v, wgu, wdn, gb, gc, vx, op,
    onehot, send, arr, gg, hd, part, r1, r2, zb, t1, t2, fin, ret,
    wgu_o, wdn_o, ggt, hdt, mg, sg,
    mixed, mx_tile, mx_halo, conv, act, cg, cg_tile, cg_halo,
    qb, qp, qs, qr, ts, tp_buf,
    in_sem, out_sem, snd, z1_sem, ag_sem, rs_sem, ret_sem, mg_sem, hl_sem, q_sem,
):
    sp = lax.axis_index("sp")
    tp = lax.axis_index("tp")
    z, core = sp // 2, lax.rem(sp, 2)
    y, x = tp // 4, lax.rem(tp, 4)
    partner = (z * 2 + 1 - core, tp)

    col = pl.ds(pl.multiple_of(tp * 128, 128), 128)
    loads = [
        pltpu.make_async_copy(moe_h.at[:, col], moe_v, in_sem.at[0]),
        pltpu.make_async_copy(cot_h, cot_v, in_sem.at[1]),
        pltpu.make_async_copy(gc_h, gc, in_sem.at[2]),
        pltpu.make_async_copy(vx_h, vx, in_sem.at[3]),
        pltpu.make_async_copy(gb_h, gb, in_sem.at[4]),
        pltpu.make_async_copy(wg_h.at[0], wgu.at[0:128], in_sem.at[5]),
        pltpu.make_async_copy(wu_h.at[0], wgu.at[128:256], in_sem.at[6]),
        pltpu.make_async_copy(wd_h.at[0], wdn, in_sem.at[7]),
        pltpu.make_async_copy(op_h, op, in_sem.at[8]),
    ]
    for c in loads:
        c.start()

    barrier = pltpu.get_barrier_semaphore()
    for b in range(1, 32):
        pl.semaphore_signal(barrier, inc=1, device_id=(lax.rem(sp + b, 32), tp), device_id_type=MESH)

    def near(dim, s):
        if dim == "x":
            return (sp, y * 4 + lax.rem(x + s + 4, 4))
        return (sp, lax.rem(y + s + 4, 4) * 4 + x)

    for dim in ("x", "y"):
        for s in (1, -1):
            pl.semaphore_signal(barrier, inc=1, device_id=near(dim, s), device_id_type=MESH)

    def push(src, dst, group, recv, dev):
        pltpu.make_async_remote_copy(
            src_ref=src, dst_ref=dst, send_sem=snd.at[group], recv_sem=recv, device_id=dev, device_id_type=MESH
        ).start()

    def landed(ref, recv):
        pltpu.make_async_remote_copy(
            src_ref=ref, dst_ref=ref, send_sem=snd.at[0], recv_sem=recv, device_id=partner, device_id_type=MESH
        ).wait_recv()

    def left(ref, group):
        pltpu.make_async_remote_copy(
            src_ref=ref, dst_ref=ref, send_sem=snd.at[group], recv_sem=z1_sem.at[0], device_id=partner,
            device_id_type=MESH,
        ).wait_send()

    def clear(i, carry):
        arr[i, :, :, CAP:SLOT] = jnp.zeros((32, 2, SLOT - CAP, 128), BF)
        return carry

    lax.fori_loop(0, 16, clear, 0)
    ret[:, CAP:SLOT] = jnp.zeros((32, SLOT - CAP, 128), BF)

    expert = lax.broadcasted_iota(jnp.int32, (32, 192), 0)
    first = (route_t[0:1, :] == expert).astype(F32)
    second = (route_t[1:2, :] == expert).astype(F32)
    before = (
        lax.broadcasted_iota(jnp.int32, (192, 192), 0) < lax.broadcasted_iota(jnp.int32, (192, 192), 1)
    ).astype(F32)
    rank = nn((first + second).astype(BF), before.astype(BF))
    spread = (
        (((lax.broadcasted_iota(jnp.int32, (32 * SLOT, 32), 0) >> 4) + sp) & 31)
        == lax.broadcasted_iota(jnp.int32, (32 * SLOT, 32), 1)
    ).astype(F32).astype(BF)
    place = (lax.broadcasted_iota(jnp.int32, (32 * SLOT, 192), 0) & (SLOT - 1)).astype(F32)
    hot0 = (nn(spread, jnp.where(first > 0, rank, -1.0).astype(BF)) == place).astype(F32)
    hot1 = (nn(spread, jnp.where(second > 0, rank, -1.0).astype(BF)) == place).astype(F32)
    onehot[...] = (hot0 + hot1).astype(BF)
    loads[0].wait()
    send[:, 0] = nn(onehot[...], moe_v[...]).astype(BF).reshape(32, SLOT, 128)
    loads[1].wait()
    cot_part = cot_v[:, col].astype(F32)
    cot0 = (weight[:, 0:1] * cot_part).astype(BF)
    cot1 = (weight[:, 1:2] * cot_part).astype(BF)
    routed = nn(hot0.astype(BF), cot0) + nn(hot1.astype(BF), cot1)
    send[:, 1] = routed.astype(BF).reshape(32, SLOT, 128)

    loads[2].wait()
    loads[3].wait()
    mixed[...] = jnp.zeros(mixed.shape, F32)
    mixed[:, 0:192] = (gc[...].astype(F32) * vx[...].astype(F32)).astype(BF).astype(F32)
    mx_tile[...] = pltpu.roll(mixed[:, 128:256], 64, 1).astype(BF)

    arr[tp, core, :, 0:CAP] = send[0, :, 0:CAP]
    pl.semaphore_wait(barrier, 35)

    order = (0, 1, -1, 2, -2, 3, -3, 4, -4, 5, -5, 6, -6, 7, -7, 8)
    for o in order:
        j = PLACE[(-o) % 16]
        zz = lax.rem(z + o + 16, 16)
        for cc in (0, 1):
            e = zz * 2 + cc
            if o == 0:
                if cc == 1:
                    continue
                e = z * 2 + 1 - core
            push(
                send.at[lax.rem(e - sp + 32, 32), :, 0:CAP], arr.at[tp, j * 2 + core, :, 0:CAP], 0,
                z1_sem.at[4 if o == 0 else j // 4], (e, tp),
            )
    after = (lax.rem(sp + 1, 32), tp)
    ahead = (lax.rem(sp + 31, 32), tp)
    push(mx_tile, mx_halo, 1, hl_sem.at[0], after)

    def z_arrived(q):
        a = 8 * q
        if q == 0:
            landed(arr.at[tp, 1 - core, :, 0:CAP], z1_sem.at[4])
            a = 2
        landed(arr.at[tp, a : 8 * q + 8, :, 0:CAP], z1_sem.at[q])

    def gather_steps(region, dims, group, sem):
        d1, d2 = dims

        def lane(a, b):
            dx, dy = (a, b) if d1 == "x" else (b, a)
            return lax.rem(y + dy + 4, 4) * 4 + lax.rem(x + dx + 4, 4)

        def half(s):
            return 0 if s == 1 else 1

        ids = {0: 0, 1: 1, -1: 2, 2: 3}

        def sem1(s):
            return sem(0 if s == 1 else 1)

        def sem2(i, s):
            return sem(3 + ids[i] * 3 + (0 if s == 1 else 1))

        def sem2f(i):
            return sem(3 + ids[i] * 3 + 2)

        def e0():
            own = region(lane(0, 0))
            for s in (1, -1):
                push(own, own, group, sem1(s), near(d1, s))
            for s in (1, -1):
                push(own, own, group, sem2(0, s), near(d2, s))

        def across(i):
            block = region(lane(i, 0))
            for s in (1, -1):
                push(block, block, group, sem2(i, s), near(d2, s))

        def on(i):
            for s in (1, -1):
                landed(region(lane(i, -s)), sem2(i, s))
                block = region(lane(i, -s), half(s))
                push(block, block, group, sem2f(i), near(d2, s))

        def e1():
            for s in (1, -1):
                landed(region(lane(-s, 0)), sem1(s))
                block = region(lane(-s, 0), half(s))
                push(block, block, group, sem(2), near(d1, s))
            for s in (1, -1):
                across(-s)
            on(0)

        def e2():
            landed(region(lane(2, 0)), sem(2))
            across(2)
            on(1)
            on(-1)

        def e3():
            on(2)

        def e4():
            for i in (0, 1, -1, 2):
                landed(region(lane(i, 2)), sem2f(i))

        return e0, e1, e2, e3, e4

    def rows_of(q):
        def region(lane, h=None):
            a, n = (8 * q, 8) if h is None else (8 * q + 4 * h, 4)
            return arr.at[lane, a : a + n, :, 0:CAP]

        return region

    dims_of = (("x", "y"), ("x", "y"), ("y", "x"), ("y", "x"))
    ag = [
        gather_steps(rows_of(q), dims_of[q], 2 + q, functools.partial(lambda q, i: ag_sem.at[q, i], q))
        for q in range(4)
    ]

    def expert_rows(q):
        a = 8 * q
        xm = jnp.concatenate([arr[l, a : a + 8, 0].reshape(128, 128) for l in range(16)], axis=1)
        pre = nt(xm, wgu[...])
        xc = jnp.concatenate([arr[l, a : a + 8, 1].reshape(128, 128) for l in range(16)], axis=1)
        hg = nt(xc, wdn[...])
        gate, up = pre[:, 0:128], pre[:, 128:256]
        sig = jax.nn.sigmoid(gate)
        silu = gate * sig
        rows = slice(128 * q, 128 * q + 128)
        hd[rows, :] = (silu * up).astype(BF)
        gg[rows, 0:128] = (hg * up * sig * (1.0 + gate * (1.0 - sig))).astype(BF)
        gg[rows, 128:256] = (hg * silu).astype(BF)
        g = gg[rows, :]
        for i in range(8):
            pv = nn(g, wgu[:, 256 * i : 256 * i + 256]).astype(BF)
            for k in (0, 1):
                l = 2 * i + k
                part[l // 4, l % 4, a : a + 8] = pv[:, 128 * k : 128 * k + 128].reshape(8, SLOT, 128)

    def back(owner):
        return lax.rem(sp - owner + 32, 32)

    def scatter_steps(q, dims):
        d1, d2 = dims
        at = {"x": x, "y": y}
        a = 8 * q

        def half(s):
            return (0, 4) if s == 1 else (4, 4)

        def bundle(d, lo=0, n=8):
            i = lax.rem(at[d1] + d + 4, 4)
            if d1 == "y":
                return part.at[i, :, a + lo : a + lo + n]
            return part.at[:, i, a + lo : a + lo + n]

        def cut(ref, dims=4):
            return ref.at[:, :, 0:CAP] if dims == 4 else ref.at[:, 0:CAP]

        def w(s):
            return 0 if s == 1 else 1

        def sem(i):
            return rs_sem.at[q, i]

        def q1():
            for s in (1, -1):
                push(cut(bundle(2, *half(s))), cut(r1.at[q, w(s)]), 6 + q, sem(w(s)), near(d1, s))

        def q2():
            for s in (1, -1):
                landed(cut(r1.at[q, w(s)]), sem(w(s)))
                mine = bundle(s, *half(s))
                mine[...] = (mine[...].astype(F32) + r1[q, w(s)].astype(F32)).astype(BF)
                push(cut(bundle(s)), cut(r2.at[q, w(s)]), 6 + q, sem(2 + w(s)), near(d1, s))

        def q3():
            for s in (1, -1):
                landed(cut(r2.at[q, w(s)]), sem(2 + w(s)))
            zb[q] = (bundle(0)[...].astype(F32) + r2[q, 0].astype(F32) + r2[q, 1].astype(F32)).astype(BF)
            i = lax.rem(at[d2] + 2, 4)
            for s in (1, -1):
                lo, n = half(s)
                push(
                    cut(zb.at[q, i, lo : lo + n], 3), cut(t1.at[q, w(s)], 3), 6 + q, sem(4 + w(s)), near(d2, s)
                )

        def q4():
            for s in (1, -1):
                landed(cut(t1.at[q, w(s)], 3), sem(4 + w(s)))
                i = lax.rem(at[d2] + s + 4, 4)
                lo, n = half(s)
                mine = zb.at[q, i, lo : lo + n]
                mine[...] = (mine[...].astype(F32) + t1[q, w(s)].astype(F32)).astype(BF)
                push(cut(zb.at[q, i], 3), cut(t2.at[q, w(s)], 3), 6 + q, sem(6 + w(s)), near(d2, s))

        def q5():
            for s in (1, -1):
                landed(cut(t2.at[q, w(s)], 3), sem(6 + w(s)))
            fin[a : a + 8] = (
                zb[q, at[d2]].astype(F32) + t2[q, 0].astype(F32) + t2[q, 1].astype(F32)
            ).astype(BF)
            for j in range(4 * q, 4 * q + 4):
                for cc in (0, 1):
                    if OFFSETS[j] == 0:
                        if cc == 0:
                            push(fin.at[1 - core, 0:CAP], ret.at[back(partner[0]), 0:CAP], 10, ret_sem, partner)
                            ret[0, 0:CAP] = fin[core, 0:CAP]
                    else:
                        dev = (lax.rem(z + OFFSETS[j] + 16, 16) * 2 + cc, tp)
                        push(fin.at[2 * j + cc, 0:CAP], ret.at[back(dev[0]), 0:CAP], 10, ret_sem, dev)

        return q1, q2, q3, q4, q5

    rs = [scatter_steps(q, dims_of[q][::-1]) for q in range(4)]

    def both(steps, c, k):
        steps[c][k]()
        steps[c + 2][k]()

    z_arrived(0)
    z_arrived(2)
    both(ag, 0, 0)
    both(ag, 0, 1)
    loads[4].wait()
    landed(mx_halo, hl_sem.at[0])
    lane_id = lax.broadcasted_iota(jnp.int32, (64, 128), 1)
    halo = jnp.where(sp == 0, 0.0, mx_halo[...].astype(F32))
    mixed[:, 128:256] = jnp.where(lane_id < 64, mixed[:, 128:256], halo)
    m = mixed[...]
    conv[...] = (
        taps[:, 2:3] * m + taps[:, 1:2] * pltpu.roll(m, 1, 1) + taps[:, 0:1] * pltpu.roll(m, 2, 1)
    )[:, 0:192]
    act[...] = (gb[...].astype(F32) * conv[...]).astype(BF)
    both(ag, 0, 2)
    z_arrived(1)
    z_arrived(3)
    both(ag, 1, 0)
    both(ag, 0, 3)
    both(ag, 1, 1)
    both(ag, 0, 4)
    for c in loads[5:8]:
        c.wait()
    expert_rows(0)
    expert_rows(2)
    both(ag, 1, 2)
    both(rs, 0, 0)
    both(ag, 1, 3)
    both(rs, 0, 1)
    both(ag, 1, 4)
    expert_rows(1)
    expert_rows(3)
    both(rs, 1, 0)
    both(rs, 0, 2)
    both(rs, 1, 1)
    both(rs, 0, 3)

    ggt[...] = gg[...].astype(F32).T.astype(BF)
    hdt[...] = hd[...].astype(F32).T.astype(BF)

    both(rs, 1, 2)
    both(rs, 0, 4)

    def weight_grads(i, carry):
        out = pl.ds(pl.multiple_of(i * 256, 256), 256)
        xm = jnp.concatenate([arr[2 * i, :, 0].reshape(512, 128), arr[2 * i + 1, :, 0].reshape(512, 128)], axis=1)
        wgu_o[:, out] = nn(ggt[...], xm).astype(BF)
        xc = jnp.concatenate([arr[2 * i, :, 1].reshape(512, 128), arr[2 * i + 1, :, 1].reshape(512, 128)], axis=1)
        wdn_o[:, out] = nn(hdt[...], xc).astype(BF)
        return carry

    both(rs, 1, 3)
    both(rs, 1, 4)
    lax.fori_loop(0, 8, weight_grads, 0)
    stores = [
        pltpu.make_async_copy(wgu_o.at[0:128], o_wg.at[0], out_sem.at[0]),
        pltpu.make_async_copy(wgu_o.at[128:256], o_wu.at[0], out_sem.at[1]),
        pltpu.make_async_copy(wdn_o, o_wd.at[0], out_sem.at[2]),
    ]
    for c in stores:
        c.start()

    landed(ret.at[1:32, 0:CAP], ret_sem)
    mine = tn(onehot[...], ret[...].reshape(32 * SLOT, 128)).astype(BF)
    mg[tp] = mine
    o_moe[...] = mine

    def tokens_of(h):
        def region(lane, k=None):
            a, n = (96 * h, 96) if k is None else (96 * h + 48 * k, 48)
            return mg.at[lane, a : a + n]

        return region

    tg = [
        gather_steps(tokens_of(h), (("x", "y"), ("y", "x"))[h], 11 + h, functools.partial(lambda h, i: mg_sem.at[h, i], h))
        for h in range(2)
    ]
    for k in range(5):
        tg[0][k]()
        tg[1][k]()

    for l in range(16):
        lanes = slice(128 * l, 128 * l + 128)
        sg[:, lanes] = (cot_v[:, lanes].astype(F32) + mg[l].astype(F32)).astype(BF)

    for i in range(8):
        pq = nn(act[...], sg[:, 256 * i : 256 * i + 256]).astype(BF)
        for k in (0, 1):
            for h in (0, 1):
                qb[h, 2 * i + k] = pq[32 * h : 32 * h + 32, 128 * k : 128 * k + 128]
    push(qb.at[1 - core], qp, 13, q_sem.at[0], partner)
    loads[8].wait()
    act_grad = nt(op[...], sg[...])
    landed(qp, q_sem.at[0])
    qs[...] = (qb[core].astype(F32) + qp[...].astype(F32)).astype(BF)
    for o in order[:0:-1]:
        zz = lax.rem(z + o + 16, 16)
        push(qs.at[zz], qr.at[PLACE[(-o) % 16]], 14, q_sem.at[1], (zz * 2 + core, tp))

    o_gb[...] = (act_grad * conv[...]).astype(BF)
    cg[...] = jnp.zeros(cg.shape, F32)
    cg[:, 0:192] = act_grad * gb[...].astype(F32)
    cg_tile[...] = pltpu.roll(cg[:, 0:128], 64, 1)
    push(cg_tile, cg_halo, 15, hl_sem.at[1], ahead)
    landed(cg_halo, hl_sem.at[1])
    later = jnp.where(sp == 31, 0.0, cg_halo[...])
    cg[:, 128:256] = jnp.where(lane_id < 64, cg[:, 128:256], later)
    g = cg[...]
    mixed_grad = (
        taps[:, 2:3] * g + taps[:, 1:2] * pltpu.roll(g, 255, 1) + taps[:, 0:1] * pltpu.roll(g, 254, 1)
    )[:, 0:192]
    o_gc[...] = (mixed_grad * vx[...].astype(F32)).astype(BF)
    o_vx[...] = (mixed_grad * gc[...].astype(F32)).astype(BF)

    total = qs[z].astype(F32)
    landed(qr.at[1:16], q_sem.at[1])
    for o in order[1:]:
        total = total + qr[PLACE[o % 16]].astype(F32)
    ts[...] = total
    push(ts, tp_buf, 16, q_sem.at[2], partner)
    landed(tp_buf, q_sem.at[2])
    low = jnp.where(core == 0, ts[...], tp_buf[...])
    high = jnp.where(core == 0, tp_buf[...], ts[...])
    for h, v in ((0, low), (1, high)):
        v = jnp.where(core == 0, v, pltpu.roll(v, 64, 1))
        o_proj[32 * h : 32 * h + 32, :] = v[:, 0:64]

    left(send.at[1:32, :, 0:CAP], 0)
    left(mx_tile, 1)
    for q in range(4):
        left(arr.at[0:15, 8 * q : 8 * q + 8, :, 0:CAP], 2 + q)
        left(arr.at[0:15, 8 * q : 8 * q + 8, 0, 0:CAP], 6 + q)
    left(ret.at[1:32, 0:CAP], 10)
    for h in range(2):
        left(mg.at[0:15, 96 * h : 96 * h + 96], 11 + h)
    left(qp, 13)
    left(qr.at[1:16], 14)
    left(cg_tile, 15)
    left(ts, 16)
    for c in stores:
        c.wait()


def on_device(
    moe_in, cotangent, routing, route_weight, w_gate, w_up, w_down, gate_b, gate_c, value_x, conv_taps, out_proj
):
    hbm = pl.BlockSpec(memory_space=pltpu.HBM)
    vmem = pl.BlockSpec(memory_space=pltpu.VMEM)
    dma = pltpu.SemaphoreType.DMA
    shape = jax.ShapeDtypeStruct
    return pl.pallas_call(
        kernel,
        out_shape=(
            shape(w_gate.shape, BF), shape(w_up.shape, BF), shape(w_down.shape, BF),
            shape((192, 128), BF), shape((64, 64), F32),
            shape((64, 192), BF), shape((64, 192), BF), shape((64, 192), BF),
        ),
        in_specs=[hbm, hbm, vmem, vmem, hbm, hbm, hbm, hbm, hbm, hbm, vmem, hbm],
        out_specs=(hbm, hbm, hbm, vmem, vmem, vmem, vmem, vmem),
        scratch_shapes=[
            VM((192, 128), BF), VM((192, 2048), BF), VM((256, 2048), BF), VM((128, 2048), BF),
            VM((64, 192), BF), VM((64, 192), BF), VM((64, 192), BF), VM((64, 2048), BF),
            VM((512, 192), BF), VM((32, 2, SLOT, 128), BF), VM((16, 32, 2, SLOT, 128), BF),
            VM((512, 256), BF), VM((512, 128), BF), VM((4, 4, 32, SLOT, 128), BF),
            VM((4, 2, 4, 4, SLOT, 128), BF), VM((4, 2, 4, 8, SLOT, 128), BF), VM((4, 4, 8, SLOT, 128), BF),
            VM((4, 2, 4, SLOT, 128), BF), VM((4, 2, 8, SLOT, 128), BF), VM((32, SLOT, 128), BF),
            VM((32, SLOT, 128), BF),
            VM((256, 2048), BF), VM((128, 2048), BF), VM((256, 512), BF), VM((128, 512), BF),
            VM((16, 192, 128), BF), VM((192, 2048), BF),
            VM((64, 256), F32), VM((64, 128), BF), VM((64, 128), BF), VM((64, 192), F32), VM((64, 192), BF),
            VM((64, 256), F32), VM((64, 128), F32), VM((64, 128), F32),
            VM((2, 16, 32, 128), BF), VM((16, 32, 128), BF), VM((16, 32, 128), BF), VM((16, 32, 128), BF),
            VM((32, 128), F32), VM((32, 128), F32),
            dma((9,)), dma((3,)), dma((17,)), dma((5,)), dma((4, 15)), dma((4, 8)), dma, dma((2, 15)), dma((2,)),
            dma((3,)),
        ],
        compiler_params=pltpu.CompilerParams(
            collective_id=0, has_side_effects=True, vmem_limit_bytes=56 * 1024 * 1024
        ),
    )(
        moe_in, cotangent, routing.T, route_weight, w_gate, w_up, w_down, gate_b, gate_c, value_x, conv_taps.T, out_proj
    )


def solution(mesh):
    in_specs = (
        P("sp", None), P("sp", None), P("sp", None), P("sp", None),
        P("sp", "tp", None), P("sp", "tp", None), P("sp", "tp", None),
        P("tp", "sp"), P("tp", "sp"), P("tp", "sp"), P(None, "tp"), P("tp", None),
    )
    out_specs = (
        P("sp", "tp", None), P("sp", "tp", None), P("sp", "tp", None),
        P("sp", "tp"), P("tp", "sp"), P("tp", "sp"), P("tp", "sp"), P("tp", "sp"),
    )
    return jax.shard_map(on_device, mesh=mesh, in_specs=in_specs, out_specs=out_specs, check_vma=False)
```

```python
import functools

import jax
import jax.numpy as jnp
from jax import lax
from jax.experimental import pallas as pl
from jax.experimental.pallas import tpu as pltpu
from jax.sharding import PartitionSpec as P

MESH = pl.DeviceIdType.MESH
BF = jnp.bfloat16
F32 = jnp.float32
VM = pltpu.VMEM

OFFSETS = (0, 1, -2, 3, -4, 5, -6, 7, -1, 2, -3, 4, -5, 6, -7, 8)
PLACE = {d % 16: j for j, d in enumerate(OFFSETS)}
SLOT = 16
CAP = 12


def nt(a, b):
    return lax.dot_general(a, b, (((1,), (1,)), ((), ())), preferred_element_type=F32)


def nn(a, b):
    return jnp.dot(a, b, preferred_element_type=F32)


def tn(a, b):
    return lax.dot_general(a, b, (((0,), (0,)), ((), ())), preferred_element_type=F32)


def kernel(
    moe_h, cot_h, route_h, weight_h, wg_h, wu_h, wd_h, gb_h, gc_h, vx_h, taps_h, op_h,
    o_wg, o_wu, o_wd, o_moe, o_proj, o_gb, o_gc, o_vx,
    route_t, weight_v, taps_v, table, turned, moe_v, cot_v, wgu, wdn, gb, gc, vx, op,
    onehot, send, arr, gg, hd, part, r1, r2, zb, t1, fin, ret,
    wgu_o, wdn_o, ggt, hdt, mixall, opt, ab, ar, qx,
    mixed, mx_tile, mx_halo, conv, act, cg, cg_tile, cg_halo,
    qb, qp, qs, qr, ts, tp_buf,
    in_sem, out_sem, snd, z1_sem, ag_sem, rs_sem, ret_sem, w_sem, hl_sem, q_sem,
):
    sp = lax.axis_index("sp")
    tp = lax.axis_index("tp")
    z, core = sp // 2, lax.rem(sp, 2)
    y, x = tp // 4, lax.rem(tp, 4)
    partner = (z * 2 + 1 - core, tp)

    def near(dim, s):
        if dim == "x":
            return (sp, y * 4 + lax.rem(x + s + 4, 4))
        return (sp, lax.rem(y + s + 4, 4) * 4 + x)

    barrier = pltpu.get_barrier_semaphore()
    order = (0, 1, -1, 2, -2, 3, -3, 4, -4, 5, -5, 6, -6, 7, -7, 8)
    for o in order[::-1]:
        zz = lax.rem(z + o + 16, 16)
        for cc in (0, 1):
            if o == 0:
                if cc == 0:
                    pl.semaphore_signal(barrier, inc=1, device_id=partner, device_id_type=MESH)
            else:
                pl.semaphore_signal(barrier, inc=1, device_id=(zz * 2 + cc, tp), device_id_type=MESH)
    for b in range(1, 16):
        pl.semaphore_signal(barrier, inc=1, device_id=(sp, lax.rem(tp + b, 16)), device_id_type=MESH)

    small = [
        pltpu.make_async_copy(route_h, route_t, in_sem.at[9]),
        pltpu.make_async_copy(weight_h, weight_v, in_sem.at[10]),
        pltpu.make_async_copy(taps_h, taps_v, in_sem.at[11]),
    ]
    for c in small:
        c.start()
    col = pl.ds(pl.multiple_of(tp * 128, 128), 128)
    loads = [
        pltpu.make_async_copy(moe_h.at[:, col], moe_v, in_sem.at[0]),
        pltpu.make_async_copy(cot_h, cot_v, in_sem.at[1]),
        pltpu.make_async_copy(gc_h, gc, in_sem.at[2]),
        pltpu.make_async_copy(vx_h, vx, in_sem.at[3]),
        pltpu.make_async_copy(gb_h, gb, in_sem.at[4]),
        pltpu.make_async_copy(wg_h.at[0], wgu.at[0:128], in_sem.at[5]),
        pltpu.make_async_copy(wu_h.at[0], wgu.at[128:256], in_sem.at[6]),
        pltpu.make_async_copy(wd_h.at[0], wdn, in_sem.at[7]),
        pltpu.make_async_copy(op_h, op, in_sem.at[8]),
    ]
    for c in loads:
        c.start()

    def push(src, dst, group, recv, dev):
        pltpu.make_async_remote_copy(
            src_ref=src, dst_ref=dst, send_sem=snd.at[group], recv_sem=recv, device_id=dev, device_id_type=MESH
        ).start()

    def landed(ref, recv):
        pltpu.make_async_remote_copy(
            src_ref=ref, dst_ref=ref, send_sem=snd.at[0], recv_sem=recv, device_id=partner, device_id_type=MESH
        ).wait_recv()

    def left(ref, group):
        pltpu.make_async_remote_copy(
            src_ref=ref, dst_ref=ref, send_sem=snd.at[group], recv_sem=z1_sem.at[0], device_id=partner,
            device_id_type=MESH,
        ).wait_send()

    def clear(i, carry):
        arr[i, :, :, CAP:SLOT] = jnp.zeros((32, 2, SLOT - CAP, 128), BF)
        return carry

    lax.fori_loop(0, 16, clear, 0)
    ret[:, CAP:SLOT] = jnp.zeros((32, SLOT - CAP, 128), BF)

    table[...] = jnp.zeros(table.shape, F32)
    for c in small:
        c.wait()
    table[0:2, 0:192] = weight_v[...]
    table[8:11, 0:64] = taps_v[...]
    turned[...] = table[...].T
    taps = [turned[0:64, 8 + j : 9 + j] for j in range(3)]

    expert = lax.broadcasted_iota(jnp.int32, (32, 192), 0)
    first = (route_t[0:1, :] == expert).astype(F32)
    second = (route_t[1:2, :] == expert).astype(F32)
    before = (
        lax.broadcasted_iota(jnp.int32, (192, 192), 0) < lax.broadcasted_iota(jnp.int32, (192, 192), 1)
    ).astype(F32)
    rank = nn((first + second).astype(BF), before.astype(BF))
    spread = (
        (((lax.broadcasted_iota(jnp.int32, (32 * SLOT, 32), 0) >> 4) + sp) & 31)
        == lax.broadcasted_iota(jnp.int32, (32 * SLOT, 32), 1)
    ).astype(F32).astype(BF)
    place = (lax.broadcasted_iota(jnp.int32, (32 * SLOT, 192), 0) & (SLOT - 1)).astype(F32)
    hot0 = (nn(spread, jnp.where(first > 0, rank, -1.0).astype(BF)) == place).astype(F32)
    hot1 = (nn(spread, jnp.where(second > 0, rank, -1.0).astype(BF)) == place).astype(F32)
    onehot[...] = (hot0 + hot1).astype(BF)
    loads[0].wait()
    send[:, 0] = nn(onehot[...], moe_v[...]).astype(BF).reshape(32, SLOT, 128)
    loads[1].wait()
    cot_part = cot_v[:, col].astype(F32)
    cot0 = (turned[0:192, 0:1] * cot_part).astype(BF)
    cot1 = (turned[0:192, 1:2] * cot_part).astype(BF)
    routed = nn(hot0.astype(BF), cot0) + nn(hot1.astype(BF), cot1)
    send[:, 1] = routed.astype(BF).reshape(32, SLOT, 128)

    loads[2].wait()
    loads[3].wait()
    mixed[...] = jnp.zeros(mixed.shape, F32)
    mixed[:, 0:192] = (gc[...].astype(F32) * vx[...].astype(F32)).astype(BF).astype(F32)
    mx_tile[...] = pltpu.roll(mixed[:, 128:256], 64, 1).astype(BF)

    arr[tp, core, :, 0:CAP] = send[0, :, 0:CAP]
    pl.semaphore_wait(barrier, 46)

    def dispatch_to(o):
        j = PLACE[(-o) % 16]
        zz = lax.rem(z + o + 16, 16)
        for cc in (0, 1):
            e = zz * 2 + cc
            if o == 0:
                if cc == 1:
                    continue
                e = z * 2 + 1 - core
            push(
                send.at[lax.rem(e - sp + 32, 32), :, 0:CAP], arr.at[tp, j * 2 + core, :, 0:CAP], 0,
                z1_sem.at[8 if o == 0 else j // 2], (e, tp),
            )

    for o in order:
        dispatch_to(o)
    after = (lax.rem(sp + 1, 32), tp)
    ahead = (lax.rem(sp + 31, 32), tp)
    push(mx_tile, mx_halo, 1, hl_sem.at[0], after)

    def z_arrived(i):
        a = 4 * i
        if i == 0:
            landed(arr.at[tp, 1 - core, :, 0:CAP], z1_sem.at[8])
            a = 2
        landed(arr.at[tp, a : 4 * i + 4, :, 0:CAP], z1_sem.at[i])

    def gather_steps(region, dims, group, sem):
        d1, d2 = dims

        def lane(a, b):
            dx, dy = (a, b) if d1 == "x" else (b, a)
            return lax.rem(y + dy + 4, 4) * 4 + lax.rem(x + dx + 4, 4)

        def half(s):
            return 0 if s == 1 else 1

        ids = {0: 0, 1: 1, -1: 2, 2: 3}

        def sem1(s):
            return sem(0 if s == 1 else 1)

        def sem2(i, s):
            return sem(3 + ids[i] * 3 + (0 if s == 1 else 1))

        def sem2f(i):
            return sem(3 + ids[i] * 3 + 2)

        def e0():
            own = region(lane(0, 0))
            for s in (1, -1):
                push(own, own, group, sem1(s), near(d1, s))
            for s in (1, -1):
                push(own, own, group, sem2(0, s), near(d2, s))

        def across(i):
            block = region(lane(i, 0))
            for s in (1, -1):
                push(block, block, group, sem2(i, s), near(d2, s))

        def on(i):
            for s in (1, -1):
                landed(region(lane(i, -s)), sem2(i, s))
                block = region(lane(i, -s), half(s))
                push(block, block, group, sem2f(i), near(d2, s))

        def e1():
            for s in (1, -1):
                landed(region(lane(-s, 0)), sem1(s))
                block = region(lane(-s, 0), half(s))
                push(block, block, group, sem(2), near(d1, s))
            for s in (1, -1):
                across(-s)
            on(0)

        def e2():
            landed(region(lane(2, 0)), sem(2))
            across(2)
            on(1)
            on(-1)

        def e3():
            on(2)

        def e4():
            for i in (0, 1, -1, 2):
                landed(region(lane(i, 2)), sem2f(i))

        return e0, e1, e2, e3, e4

    def rows_of(q):
        def region(lane, h=None):
            a, n = (4 * q, 4) if h is None else (4 * q + 2 * h, 2)
            return arr.at[lane, a : a + n, :, 0:CAP]

        return region

    dims_of = (("x", "y"), ("x", "y"), ("y", "x"), ("y", "x"))
    ag = [
        gather_steps(rows_of(i), dims_of[i // 2], 2 + i, functools.partial(lambda i, k: ag_sem.at[i, k], i))
        for i in range(8)
    ]

    def expert_rows(q):
        a = 8 * q
        xm = jnp.concatenate([arr[l, a : a + 8, 0].reshape(128, 128) for l in range(16)], axis=1)
        pre = nt(xm, wgu[...])
        xc = jnp.concatenate([arr[l, a : a + 8, 1].reshape(128, 128) for l in range(16)], axis=1)
        hg = nt(xc, wdn[...])
        gate, up = pre[:, 0:128], pre[:, 128:256]
        sig = jax.nn.sigmoid(gate)
        silu = gate * sig
        rows = slice(128 * q, 128 * q + 128)
        hd[rows, :] = (silu * up).astype(BF)
        gg[rows, 0:128] = (hg * up * sig * (1.0 + gate * (1.0 - sig))).astype(BF)
        gg[rows, 128:256] = (hg * silu).astype(BF)
        g = gg[rows, :]
        for i in range(8):
            pv = nn(g, wgu[:, 256 * i : 256 * i + 256]).astype(BF)
            for k in (0, 1):
                l = 2 * i + k
                part[l // 4, l % 4, a : a + 8] = pv[:, 128 * k : 128 * k + 128].reshape(8, SLOT, 128)

    def back(owner):
        return lax.rem(sp - owner + 32, 32)

    def scatter_steps(q, dims):
        d1, d2 = dims
        at = {"x": x, "y": y}
        a = 8 * q

        def half(s):
            return (0, 4) if s == 1 else (4, 4)

        def bundle(d, lo=0, n=8):
            i = lax.rem(at[d1] + d + 4, 4)
            if d1 == "y":
                return part.at[i, :, a + lo : a + lo + n]
            return part.at[:, i, a + lo : a + lo + n]

        def cut(ref, dims=4):
            return ref.at[:, :, 0:CAP] if dims == 4 else ref.at[:, 0:CAP]

        def w(s):
            return 0 if s == 1 else 1

        def sem(i):
            return rs_sem.at[q, i]

        def q1():
            for s in (1, -1):
                push(cut(bundle(2, *half(s))), cut(r1.at[q, w(s)]), 10 + q, sem(w(s)), near(d1, s))

        def q2():
            for s in (1, -1):
                landed(cut(r1.at[q, w(s)]), sem(w(s)))
                mine = bundle(s, *half(s))
                mine[...] = (mine[...].astype(F32) + r1[q, w(s)].astype(F32)).astype(BF)
                push(cut(bundle(s)), cut(r2.at[q, w(s)]), 10 + q, sem(2 + w(s)), near(d1, s))

        def q3():
            for s in (1, -1):
                landed(cut(r2.at[q, w(s)]), sem(2 + w(s)))
            zb[q] = (bundle(0)[...].astype(F32) + r2[q, 0].astype(F32) + r2[q, 1].astype(F32)).astype(BF)
            for k, s in enumerate((2, 1, -1)):
                i = lax.rem(at[d2] + s + 4, 4)
                push(cut(zb.at[q, i], 3), cut(t1.at[q, k], 3), 10 + q, sem(4 + k), near(d2, s))

        def q4():
            for k in range(3):
                landed(cut(t1.at[q, k], 3), sem(4 + k))
            fin[a : a + 8] = (
                zb[q, at[d2]].astype(F32) + t1[q, 0].astype(F32) + t1[q, 1].astype(F32) + t1[q, 2].astype(F32)
            ).astype(BF)
            for j in range(4 * q + 3, 4 * q - 1, -1):
                for cc in (0, 1):
                    if OFFSETS[j] == 0:
                        if cc == 0:
                            push(fin.at[1 - core, 0:CAP], ret.at[back(partner[0]), 0:CAP], 14, ret_sem, partner)
                            ret[0, 0:CAP] = fin[core, 0:CAP]
                    else:
                        dev = (lax.rem(z + OFFSETS[j] + 16, 16) * 2 + cc, tp)
                        push(fin.at[2 * j + cc, 0:CAP], ret.at[back(dev[0]), 0:CAP], 14, ret_sem, dev)

        return q1, q2, q3, q4

    rs = [scatter_steps(q, dims_of[q][::-1]) for q in range(4)]

    def both(steps, c, k):
        steps[c][k]()
        steps[c + len(steps) // 2][k]()

    z_arrived(0)
    z_arrived(4)
    both(ag, 0, 0)
    z_arrived(1)
    z_arrived(5)
    both(ag, 1, 0)
    both(ag, 0, 1)
    z_arrived(2)
    z_arrived(6)
    both(ag, 2, 0)
    loads[4].wait()
    landed(mx_halo, hl_sem.at[0])
    lane_id = lax.broadcasted_iota(jnp.int32, (64, 128), 1)
    halo = jnp.where(sp == 0, 0.0, mx_halo[...].astype(F32))
    mixed[:, 128:256] = jnp.where(lane_id < 64, mixed[:, 128:256], halo)
    m = mixed[...]
    conv[...] = (
        taps[2] * m + taps[1] * pltpu.roll(m, 1, 1) + taps[0] * pltpu.roll(m, 2, 1)
    )[:, 0:192]
    act[...] = (gb[...].astype(F32) * conv[...]).astype(BF)
    for c in loads[5:9]:
        c.wait()
    both(ag, 1, 1)
    z_arrived(3)
    z_arrived(7)
    both(ag, 3, 0)
    both(ag, 0, 2)
    both(ag, 2, 1)
    both(ag, 1, 2)
    both(ag, 3, 1)
    both(ag, 0, 3)
    both(ag, 2, 2)
    both(ag, 1, 3)
    both(ag, 0, 4)
    both(ag, 3, 2)
    both(ag, 2, 3)
    both(ag, 1, 4)
    both(ag, 3, 3)
    expert_rows(0)
    expert_rows(2)
    both(rs, 0, 0)
    both(ag, 2, 4)
    both(ag, 3, 4)
    expert_rows(1)
    expert_rows(3)
    both(rs, 1, 0)
    both(rs, 0, 1)
    both(rs, 1, 1)
    both(rs, 0, 2)
    both(rs, 1, 2)
    both(rs, 0, 3)

    ggt[...] = gg[...].astype(F32).T.astype(BF)
    hdt[...] = hd[...].astype(F32).T.astype(BF)

    def weight_grads(i, carry):
        out = pl.ds(pl.multiple_of(i * 256, 256), 256)
        xm = jnp.concatenate([arr[2 * i, :, 0].reshape(512, 128), arr[2 * i + 1, :, 0].reshape(512, 128)], axis=1)
        wgu_o[:, out] = nn(ggt[...], xm).astype(BF)
        xc = jnp.concatenate([arr[2 * i, :, 1].reshape(512, 128), arr[2 * i + 1, :, 1].reshape(512, 128)], axis=1)
        wdn_o[:, out] = nn(hdt[...], xc).astype(BF)
        return carry

    both(rs, 1, 3)

    mixall[0] = act[...]
    opt[0] = op[:, col]
    for b in range(1, 16):
        lane = lax.rem(tp + b, 16)
        push(act, mixall.at[16 - b], 15, w_sem.at[0], (sp, lane))
    for b in range(1, 16):
        lane = lax.rem(tp + b, 16)
        there = pl.ds(pl.multiple_of(lane * 128, 128), 128)
        push(op.at[:, there], opt.at[16 - b], 16, w_sem.at[1], (sp, lane))
    lax.fori_loop(0, 8, weight_grads, 0)
    stores = [
        pltpu.make_async_copy(wgu_o.at[0:128], o_wg.at[0], out_sem.at[0]),
        pltpu.make_async_copy(wgu_o.at[128:256], o_wu.at[0], out_sem.at[1]),
        pltpu.make_async_copy(wdn_o, o_wd.at[0], out_sem.at[2]),
    ]
    for c in stores:
        c.start()

    landed(ret.at[1:32, 0:CAP], ret_sem)
    mine = tn(onehot[...], ret[...].reshape(32 * SLOT, 128)).astype(BF)
    o_moe[...] = mine
    stream = (cot_v[:, col].astype(F32) + mine.astype(F32)).astype(BF)

    landed(mixall.at[1:16], w_sem.at[0])
    for i in range(4):
        pq = nn(mixall[4 * i : 4 * i + 4].reshape(256, 192), stream).astype(BF).reshape(4, 2, 32, 128)
        for h in (0, 1):
            qb[h, 4 * i : 4 * i + 4] = pq[:, h]
    push(qb.at[1 - core], qp, 17, q_sem.at[0], partner)
    landed(opt.at[1:16], w_sem.at[1])
    for i in range(4):
        pa = nt(opt[4 * i : 4 * i + 4].reshape(256, 128), stream).astype(BF)
        ab[4 * i : 4 * i + 4] = pa.reshape(4, 64, 192)
    landed(qp, q_sem.at[0])
    qs[...] = (qb[core].astype(F32) + qp[...].astype(F32)).astype(BF)
    qx[0] = qs[0]
    for b in range(1, 16):
        push(qs.at[b], qx.at[16 - b], 18, q_sem.at[3], (sp, lax.rem(tp + b, 16)))
    for b in range(1, 16):
        push(ab.at[b], ar.at[16 - b], 19, w_sem.at[2], (sp, lax.rem(tp + b, 16)))
    landed(qx.at[1:16], q_sem.at[3])
    for o in order[:0:-1]:
        zz = lax.rem(z + o + 16, 16)
        push(
            qx.at[lax.rem(zz - tp + 16, 16)], qr.at[PLACE[(-o) % 16]], 20, q_sem.at[1], (zz * 2 + core, tp)
        )
    landed(ar.at[1:16], w_sem.at[2])
    act_grad = ab[0].astype(F32)
    for b in range(1, 16):
        act_grad = act_grad + ar[b].astype(F32)

    o_gb[...] = (act_grad * conv[...]).astype(BF)
    cg[...] = jnp.zeros(cg.shape, F32)
    cg[:, 0:192] = act_grad * gb[...].astype(F32)
    cg_tile[...] = pltpu.roll(cg[:, 0:128], 64, 1)
    push(cg_tile, cg_halo, 21, hl_sem.at[1], ahead)
    landed(cg_halo, hl_sem.at[1])
    later = jnp.where(sp == 31, 0.0, cg_halo[...])
    cg[:, 128:256] = jnp.where(lane_id < 64, cg[:, 128:256], later)
    g = cg[...]
    mixed_grad = (
        taps[2] * g + taps[1] * pltpu.roll(g, 255, 1) + taps[0] * pltpu.roll(g, 254, 1)
    )[:, 0:192]
    o_gc[...] = (mixed_grad * vx[...].astype(F32)).astype(BF)
    o_vx[...] = (mixed_grad * gc[...].astype(F32)).astype(BF)

    total = qx[lax.rem(z - tp + 16, 16)].astype(F32)
    landed(qr.at[1:16], q_sem.at[1])
    for o in order[1:]:
        total = total + qr[PLACE[o % 16]].astype(F32)
    ts[...] = total
    push(ts, tp_buf, 22, q_sem.at[2], partner)
    landed(tp_buf, q_sem.at[2])
    low = jnp.where(core == 0, ts[...], tp_buf[...])
    high = jnp.where(core == 0, tp_buf[...], ts[...])
    for h, v in ((0, low), (1, high)):
        v = jnp.where(core == 0, v, pltpu.roll(v, 64, 1))
        o_proj[32 * h : 32 * h + 32, :] = v[:, 0:64]

    left(send.at[1:32, :, 0:CAP], 0)
    left(mx_tile, 1)
    for i in range(8):
        left(arr.at[0:15, 4 * i : 4 * i + 4, :, 0:CAP], 2 + i)
    for q in range(4):
        left(arr.at[0:15, 8 * q : 8 * q + 8, 0, 0:CAP], 10 + q)
    left(ret.at[1:32, 0:CAP], 14)
    left(mixall.at[1:16], 15)
    left(opt.at[1:16], 16)
    left(qp, 17)
    left(qx.at[1:16], 18)
    left(ar.at[1:16], 19)
    left(qr.at[1:16], 20)
    left(cg_tile, 21)
    left(ts, 22)
    for c in stores:
        c.wait()


def copy_kernel(*refs):
    ins, outs, rest = refs[:8], refs[8:16], refs[16:]
    bufs, sem_in, sem_out = rest[:8], rest[8], rest[9]
    reads = [pltpu.make_async_copy(a, b, sem_in.at[i]) for i, (a, b) in enumerate(zip(ins, bufs))]
    writes = [pltpu.make_async_copy(b, o, sem_out.at[i]) for i, (b, o) in enumerate(zip(bufs, outs))]
    for c in reads:
        c.start()
    for r, w in zip(reads, writes):
        r.wait()
        w.start()
    for w in writes:
        w.wait()


def handed_out(arrays):
    hbm = pl.BlockSpec(memory_space=pltpu.HBM)
    return pl.pallas_call(
        copy_kernel,
        out_shape=tuple(jax.ShapeDtypeStruct(a.shape, a.dtype) for a in arrays),
        in_specs=[hbm] * 8,
        out_specs=tuple([hbm] * 8),
        scratch_shapes=[VM(a.shape, a.dtype) for a in arrays]
        + [pltpu.SemaphoreType.DMA((8,)), pltpu.SemaphoreType.DMA((8,))],
    )(*arrays)


def on_device(
    moe_in, cotangent, routing, route_weight, w_gate, w_up, w_down, gate_b, gate_c, value_x, conv_taps, out_proj
):
    hbm = pl.BlockSpec(memory_space=pltpu.HBM)
    vmem = pl.BlockSpec(memory_space=pltpu.VMEM)
    dma = pltpu.SemaphoreType.DMA
    shape = jax.ShapeDtypeStruct
    grads = pl.pallas_call(
        kernel,
        out_shape=(
            shape(w_gate.shape, BF), shape(w_up.shape, BF), shape(w_down.shape, BF),
            shape((192, 128), BF), shape((64, 64), F32),
            shape((64, 192), BF), shape((64, 192), BF), shape((64, 192), BF),
        ),
        in_specs=[hbm] * 12,
        out_specs=(hbm, hbm, hbm, vmem, vmem, vmem, vmem, vmem),
        scratch_shapes=[
            VM((2, 192), jnp.int32), VM((2, 192), F32), VM((3, 64), F32), VM((128, 256), F32), VM((256, 128), F32),
            VM((192, 128), BF), VM((192, 2048), BF), VM((256, 2048), BF), VM((128, 2048), BF),
            VM((64, 192), BF), VM((64, 192), BF), VM((64, 192), BF), VM((64, 2048), BF),
            VM((512, 192), BF), VM((32, 2, SLOT, 128), BF), VM((16, 32, 2, SLOT, 128), BF),
            VM((512, 256), BF), VM((512, 128), BF), VM((4, 4, 32, SLOT, 128), BF),
            VM((4, 2, 4, 4, SLOT, 128), BF), VM((4, 2, 4, 8, SLOT, 128), BF), VM((4, 4, 8, SLOT, 128), BF),
            VM((4, 3, 8, SLOT, 128), BF), VM((32, SLOT, 128), BF),
            VM((32, SLOT, 128), BF),
            VM((256, 2048), BF), VM((128, 2048), BF), VM((256, 512), BF), VM((128, 512), BF),
            VM((16, 64, 192), BF), VM((16, 64, 128), BF), VM((16, 64, 192), BF), VM((16, 64, 192), BF), VM((16, 32, 128), BF),
            VM((64, 256), F32), VM((64, 128), BF), VM((64, 128), BF), VM((64, 192), F32), VM((64, 192), BF),
            VM((64, 256), F32), VM((64, 128), F32), VM((64, 128), F32),
            VM((2, 16, 32, 128), BF), VM((16, 32, 128), BF), VM((16, 32, 128), BF), VM((16, 32, 128), BF),
            VM((32, 128), F32), VM((32, 128), F32),
            dma((12,)), dma((3,)), dma((23,)), dma((9,)), dma((8, 15)), dma((4, 7)), dma, dma((3,)), dma((2,)),
            dma((4,)),
        ],
        compiler_params=pltpu.CompilerParams(
            collective_id=0, has_side_effects=True, vmem_limit_bytes=56 * 1024 * 1024
        ),
    )(
        moe_in, cotangent, routing.T, route_weight.T, w_gate, w_up, w_down, gate_b, gate_c, value_x, conv_taps, out_proj
    )
    return handed_out(grads)


def solution(mesh):
    in_specs = (
        P("sp", None), P("sp", None), P("sp", None), P("sp", None),
        P("sp", "tp", None), P("sp", "tp", None), P("sp", "tp", None),
        P("tp", "sp"), P("tp", "sp"), P("tp", "sp"), P(None, "tp"), P("tp", None),
    )
    out_specs = (
        P("sp", "tp", None), P("sp", "tp", None), P("sp", "tp", None),
        P("sp", "tp"), P("tp", "sp"), P("tp", "sp"), P("tp", "sp"), P("tp", "sp"),
    )
    return jax.shard_map(on_device, mesh=mesh, in_specs=in_specs, out_specs=out_specs, check_vma=False)
```

```python
import functools

import jax
import jax.numpy as jnp
from jax import lax
from jax.experimental import pallas as pl
from jax.experimental.pallas import tpu as pltpu
from jax.sharding import PartitionSpec as P

MESH = pl.DeviceIdType.MESH
BF = jnp.bfloat16
F32 = jnp.float32
VM = pltpu.VMEM

OFFSETS = (0, 1, -2, 3, -4, 5, -6, 7, -1, 2, -3, 4, -5, 6, -7, 8)
PLACE = {d % 16: j for j, d in enumerate(OFFSETS)}
SLOT = 16
CAP = 12


def nt(a, b):
    return lax.dot_general(a, b, (((1,), (1,)), ((), ())), preferred_element_type=F32)


def nn(a, b):
    return jnp.dot(a, b, preferred_element_type=F32)


def tn(a, b):
    return lax.dot_general(a, b, (((0,), (0,)), ((), ())), preferred_element_type=F32)


def kernel(
    moe_h, cot_h, route_h, weight_h, wg_h, wu_h, wd_h, gb_h, gc_h, vx_h, taps_h, op_h,
    o_wg, o_wu, o_wd, o_moe, o_proj, o_gb, o_gc, o_vx,
    route_t, weight_v, taps_v, table, turned, moe_v, cot_v, wgu, wdn, gb, gc, vx, op,
    onehot, send, arr, gg, hd, part, r1, r2, r3, zb, t1, fin, ret,
    ggt, hdt, mixall, opt, ab, ar, qx,
    mixed, mx_tile, mx_halo, conv, act, cg, cg_tile, cg_halo,
    qb, qp, qs, qr, ts, tp_buf,
    in_sem, snd, z1_sem, ag_sem, rs_sem, ret_sem, w_sem, hl_sem, q_sem,
):
    sp = lax.axis_index("sp")
    tp = lax.axis_index("tp")
    z, core = sp // 2, lax.rem(sp, 2)
    y, x = tp // 4, lax.rem(tp, 4)
    partner = (z * 2 + 1 - core, tp)

    def near(dim, s):
        if dim == "x":
            return (sp, y * 4 + lax.rem(x + s + 4, 4))
        return (sp, lax.rem(y + s + 4, 4) * 4 + x)

    barrier = pltpu.get_barrier_semaphore()
    order = (0, 1, -1, 2, -2, 3, -3, 4, -4, 5, -5, 6, -6, 7, -7, 8)
    for o in order[::-1]:
        zz = lax.rem(z + o + 16, 16)
        for cc in (0, 1):
            if o == 0:
                if cc == 0:
                    pl.semaphore_signal(barrier, inc=1, device_id=partner, device_id_type=MESH)
            else:
                pl.semaphore_signal(barrier, inc=1, device_id=(zz * 2 + cc, tp), device_id_type=MESH)
    for b in range(1, 16):
        pl.semaphore_signal(barrier, inc=1, device_id=(sp, lax.rem(tp + b, 16)), device_id_type=MESH)

    small = [
        pltpu.make_async_copy(route_h, route_t, in_sem.at[9]),
        pltpu.make_async_copy(weight_h, weight_v, in_sem.at[10]),
        pltpu.make_async_copy(taps_h, taps_v, in_sem.at[11]),
    ]
    for c in small:
        c.start()
    col = pl.ds(pl.multiple_of(tp * 128, 128), 128)
    loads = [
        pltpu.make_async_copy(moe_h.at[:, col], moe_v, in_sem.at[0]),
        pltpu.make_async_copy(cot_h, cot_v, in_sem.at[1]),
        pltpu.make_async_copy(gc_h, gc, in_sem.at[2]),
        pltpu.make_async_copy(vx_h, vx, in_sem.at[3]),
        pltpu.make_async_copy(gb_h, gb, in_sem.at[4]),
        pltpu.make_async_copy(wg_h.at[0], wgu.at[0:128], in_sem.at[5]),
        pltpu.make_async_copy(wu_h.at[0], wgu.at[128:256], in_sem.at[6]),
        pltpu.make_async_copy(wd_h.at[0], wdn, in_sem.at[7]),
        pltpu.make_async_copy(op_h, op, in_sem.at[8]),
    ]
    for c in loads:
        c.start()

    def push(src, dst, group, recv, dev):
        pltpu.make_async_remote_copy(
            src_ref=src, dst_ref=dst, send_sem=snd.at[group], recv_sem=recv, device_id=dev, device_id_type=MESH
        ).start()

    def landed(ref, recv):
        pltpu.make_async_remote_copy(
            src_ref=ref, dst_ref=ref, send_sem=snd.at[0], recv_sem=recv, device_id=partner, device_id_type=MESH
        ).wait_recv()

    def left(ref, group):
        pltpu.make_async_remote_copy(
            src_ref=ref, dst_ref=ref, send_sem=snd.at[group], recv_sem=z1_sem.at[0], device_id=partner,
            device_id_type=MESH,
        ).wait_send()

    def clear(i, carry):
        arr[i, :, :, CAP:SLOT] = jnp.zeros((32, 2, SLOT - CAP, 128), BF)
        return carry

    lax.fori_loop(0, 16, clear, 0)
    ret[:, CAP:SLOT] = jnp.zeros((32, SLOT - CAP, 128), BF)

    table[...] = jnp.zeros(table.shape, F32)
    for c in small:
        c.wait()
    table[0:2, 0:192] = weight_v[...]
    table[8:11, 0:64] = taps_v[...]
    turned[...] = table[...].T
    taps = [turned[0:64, 8 + j : 9 + j] for j in range(3)]

    expert = lax.broadcasted_iota(jnp.int32, (32, 192), 0)
    first = (route_t[0:1, :] == expert).astype(F32)
    second = (route_t[1:2, :] == expert).astype(F32)
    before = (
        lax.broadcasted_iota(jnp.int32, (192, 192), 0) < lax.broadcasted_iota(jnp.int32, (192, 192), 1)
    ).astype(F32)
    rank = nn((first + second).astype(BF), before.astype(BF))
    spread = (
        (((lax.broadcasted_iota(jnp.int32, (32 * SLOT, 32), 0) >> 4) + sp) & 31)
        == lax.broadcasted_iota(jnp.int32, (32 * SLOT, 32), 1)
    ).astype(F32).astype(BF)
    place = (lax.broadcasted_iota(jnp.int32, (32 * SLOT, 192), 0) & (SLOT - 1)).astype(F32)
    hot0 = (nn(spread, jnp.where(first > 0, rank, -1.0).astype(BF)) == place).astype(F32)
    hot1 = (nn(spread, jnp.where(second > 0, rank, -1.0).astype(BF)) == place).astype(F32)
    onehot[...] = (hot0 + hot1).astype(BF)
    loads[0].wait()
    send[:, 0] = nn(onehot[...], moe_v[...]).astype(BF).reshape(32, SLOT, 128)
    loads[1].wait()
    cot_part = cot_v[:, col].astype(F32)
    cot0 = (turned[0:192, 0:1] * cot_part).astype(BF)
    cot1 = (turned[0:192, 1:2] * cot_part).astype(BF)
    routed = nn(hot0.astype(BF), cot0) + nn(hot1.astype(BF), cot1)
    send[:, 1] = routed.astype(BF).reshape(32, SLOT, 128)

    loads[2].wait()
    loads[3].wait()
    mixed[...] = jnp.zeros(mixed.shape, F32)
    mixed[:, 0:192] = (gc[...].astype(F32) * vx[...].astype(F32)).astype(BF).astype(F32)
    mx_tile[...] = pltpu.roll(mixed[:, 128:256], 64, 1).astype(BF)

    arr[tp, core, :, 0:CAP] = send[0, :, 0:CAP]
    pl.semaphore_wait(barrier, 46)

    def dispatch_to(o):
        j = PLACE[(-o) % 16]
        zz = lax.rem(z + o + 16, 16)
        for cc in (0, 1):
            e = zz * 2 + cc
            if o == 0:
                if cc == 1:
                    continue
                e = z * 2 + 1 - core
            push(
                send.at[lax.rem(e - sp + 32, 32), :, 0:CAP], arr.at[tp, j * 2 + core, :, 0:CAP], 0,
                z1_sem.at[8 if o == 0 else j // 2], (e, tp),
            )

    def dispatch(*chunks):
        for o in order:
            if PLACE[(-o) % 16] % 8 // 2 in chunks:
                dispatch_to(o)

    dispatch(0, 1)
    after = (lax.rem(sp + 1, 32), tp)
    ahead = (lax.rem(sp + 31, 32), tp)
    push(mx_tile, mx_halo, 1, hl_sem.at[0], after)

    def z_arrived(i):
        a = 4 * i
        if i == 0:
            landed(arr.at[tp, 1 - core, :, 0:CAP], z1_sem.at[8])
            a = 2
        landed(arr.at[tp, a : 4 * i + 4, :, 0:CAP], z1_sem.at[i])

    def gather_steps(region, dims, group, sem, direct):
        d1, d2 = dims

        def lane(a, b):
            dx, dy = (a, b) if d1 == "x" else (b, a)
            return lax.rem(y + dy + 4, 4) * 4 + lax.rem(x + dx + 4, 4)

        def half(s):
            return 0 if s == 1 else 1

        ids = {0: 0, 1: 1, -1: 2, 2: 3}

        def sem1(s):
            return sem(0 if s == 1 else 1)

        def sem2(i, s):
            return sem(3 + ids[i] * 3 + (0 if s == 1 else 1))

        def sem2f(i):
            return sem(3 + ids[i] * 3 + 2)

        def e0():
            own = region(lane(0, 0))
            for s in (1, -1):
                push(own, own, group, sem1(s), near(d1, s))
            if direct:
                push(own, own, group, sem(2), near(d1, 2))
            for s in (1, -1):
                push(own, own, group, sem2(0, s), near(d2, s))

        def across(i):
            block = region(lane(i, 0))
            for s in (1, -1):
                push(block, block, group, sem2(i, s), near(d2, s))

        def on(i):
            for s in (1, -1):
                landed(region(lane(i, -s)), sem2(i, s))
                block = region(lane(i, -s), half(s))
                push(block, block, group, sem2f(i), near(d2, s))

        def e1():
            for s in (1, -1):
                landed(region(lane(-s, 0)), sem1(s))
                if not direct:
                    block = region(lane(-s, 0), half(s))
                    push(block, block, group, sem(2), near(d1, s))
            for s in (1, -1):
                across(-s)
            on(0)

        def e2():
            landed(region(lane(2, 0)), sem(2))
            across(2)

        def e3():
            on(1)
            on(-1)
            on(2)

        def e4():
            for i in (0, 1, -1, 2):
                landed(region(lane(i, 2)), sem2f(i))

        return e0, e1, e2, e3, e4

    def rows_of(q):
        def region(lane, h=None):
            a, n = (4 * q, 4) if h is None else (4 * q + 2 * h, 2)
            return arr.at[lane, a : a + n, :, 0:CAP]

        return region

    dims_of = (("x", "y"), ("x", "y"), ("y", "x"), ("y", "x"))
    ag = [
        gather_steps(rows_of(i), dims_of[i // 2], 2 + i, functools.partial(lambda i, k: ag_sem.at[i, k], i), True)
        for i in range(8)
    ]

    def expert_rows(c):
        parts = (4 * c, 4 * c + 16)

        def wide(kind):
            return jnp.concatenate(
                [
                    jnp.concatenate([arr[l, a : a + 4, kind].reshape(64, 128) for a in parts], axis=0)
                    for l in range(16)
                ],
                axis=1,
            )

        pre = nt(wide(0), wgu[...])
        hg = nt(wide(1), wdn[...])
        gate, up = pre[:, 0:128], pre[:, 128:256]
        sig = jax.nn.sigmoid(gate)
        silu = gate * sig
        hidden = (silu * up).astype(BF)
        g = jnp.concatenate([hg * up * sig * (1.0 + gate * (1.0 - sig)), hg * silu], axis=1).astype(BF)
        for h, a in enumerate(parts):
            hd[16 * a : 16 * a + 64, :] = hidden[64 * h : 64 * h + 64]
            gg[16 * a : 16 * a + 64, :] = g[64 * h : 64 * h + 64]
        for i in range(8):
            pv = nn(g, wgu[:, 256 * i : 256 * i + 256]).astype(BF)
            for k in (0, 1):
                l = 2 * i + k
                for h, a in enumerate(parts):
                    part[l // 4, l % 4, a : a + 4] = pv[
                        64 * h : 64 * h + 64, 128 * k : 128 * k + 128
                    ].reshape(4, SLOT, 128)

    def back(owner):
        return lax.rem(sp - owner + 32, 32)

    def scatter_steps(q, dims):
        d1, d2 = dims
        at = {"x": x, "y": y}
        a = 4 * q

        def half(s):
            return (0, 2) if s == 1 else (2, 2)

        def bundle(d, lo=0, n=4):
            i = lax.rem(at[d1] + d + 4, 4)
            if d1 == "y":
                return part.at[i, :, a + lo : a + lo + n]
            return part.at[:, i, a + lo : a + lo + n]

        def cut(ref, dims=4):
            return ref.at[:, :, 0:CAP] if dims == 4 else ref.at[:, 0:CAP]

        def w(s):
            return 0 if s == 1 else 1

        def sem(i):
            return rs_sem.at[q, i]

        direct = q % 4 == 3

        def q1():
            if direct:
                push(cut(bundle(2)), cut(r3.at[q // 4]), 10 + q, sem(0), near(d1, 2))
                for s in (1, -1):
                    push(cut(bundle(s)), cut(r2.at[q, w(s)]), 10 + q, sem(2 + w(s)), near(d1, s))
                return
            for s in (1, -1):
                push(cut(bundle(2, *half(s))), cut(r1.at[q, w(s)]), 10 + q, sem(w(s)), near(d1, s))

        def q2():
            if direct:
                return
            for s in (1, -1):
                landed(cut(r1.at[q, w(s)]), sem(w(s)))
                mine = bundle(s, *half(s))
                mine[...] = (mine[...].astype(F32) + r1[q, w(s)].astype(F32)).astype(BF)
                push(cut(bundle(s)), cut(r2.at[q, w(s)]), 10 + q, sem(2 + w(s)), near(d1, s))

        def q3():
            for s in (1, -1):
                landed(cut(r2.at[q, w(s)]), sem(2 + w(s)))
            own = bundle(0)[...].astype(F32)
            if direct:
                landed(cut(r3.at[q // 4]), sem(0))
                own = own + r3[q // 4].astype(F32)
            zb[q] = (own + r2[q, 0].astype(F32) + r2[q, 1].astype(F32)).astype(BF)
            for k, s in enumerate((2, 1, -1)):
                i = lax.rem(at[d2] + s + 4, 4)
                push(cut(zb.at[q, i], 3), cut(t1.at[q, k], 3), 10 + q, sem(4 + k), near(d2, s))

        def q4():
            for k in range(3):
                landed(cut(t1.at[q, k], 3), sem(4 + k))
            fin[a : a + 4] = (
                zb[q, at[d2]].astype(F32) + t1[q, 0].astype(F32) + t1[q, 1].astype(F32) + t1[q, 2].astype(F32)
            ).astype(BF)
            for j in (2 * q + 1, 2 * q):
                for cc in (0, 1):
                    if OFFSETS[j] == 0:
                        if cc == 0:
                            push(fin.at[1 - core, 0:CAP], ret.at[back(partner[0]), 0:CAP], 18, ret_sem, partner)
                            ret[0, 0:CAP] = fin[core, 0:CAP]
                    else:
                        dev = (lax.rem(z + OFFSETS[j] + 16, 16) * 2 + cc, tp)
                        push(fin.at[2 * j + cc, 0:CAP], ret.at[back(dev[0]), 0:CAP], 18, ret_sem, dev)

        return q1, q2, q3, q4

    rs = [scatter_steps(i, dims_of[i // 2][::-1]) for i in range(8)]

    def both(steps, c, k):
        steps[c][k]()
        steps[c + len(steps) // 2][k]()

    lane_id = lax.broadcasted_iota(jnp.int32, (64, 128), 1)

    def start(i):
        z_arrived(i)
        ag[i][0]()
        if i == 0:
            dispatch(2, 3)

    def step(steps, i, k):
        steps[i][k]()

    def forward():
        loads[4].wait()
        landed(mx_halo, hl_sem.at[0])
        halo = jnp.where(sp == 0, 0.0, mx_halo[...].astype(F32))
        mixed[:, 128:256] = jnp.where(lane_id < 64, mixed[:, 128:256], halo)
        m = mixed[...]
        conv[...] = (
            taps[2] * m + taps[1] * pltpu.roll(m, 1, 1) + taps[0] * pltpu.roll(m, 2, 1)
        )[:, 0:192]
        act[...] = (gb[...].astype(F32) * conv[...]).astype(BF)
        for c in loads[5:9]:
            c.wait()

    def rows(c):
        both(ag, c, 4)
        expert_rows(c)
        both(rs, c, 0)

    plane = sorted(
        ((dy, dx) for dy in range(4) for dx in range(4) if (dy, dx) != (0, 0)),
        key=lambda d: -(min(d[0], 4 - d[0]) + min(d[1], 4 - d[1])),
    )

    def lanes():
        for dy, dx in plane:
            lane = lax.rem(y + dy, 4) * 4 + lax.rem(x + dx, 4)
            yield lane, lax.rem(lane - tp + 16, 16)

    def exchange():
        mixall[0] = act[...]
        opt[0] = op[:, col]
        for lane, b in lanes():
            push(act, mixall.at[16 - b], 19, w_sem.at[0], (sp, lane))
        for lane, b in lanes():
            there = pl.ds(pl.multiple_of(lane * 128, 128), 128)
            push(op.at[:, there], opt.at[16 - b], 20, w_sem.at[1], (sp, lane))

    due = [(17.3, forward), (46.0, exchange)]
    for i, t in enumerate((10.7, 13.5, 16.5, 20.0, 12.0, 15.0, 17.5, 20.8)):
        due.append((t, functools.partial(start, i)))
        for k, dt in ((1, 4.2), (2, 4.8), (3, 9.0)):
            due.append((t + dt, functools.partial(step, ag, i, k)))
    for c, t in enumerate((26.5, 29.5, 32.0, 33.5)):
        due.append((t, functools.partial(rows, c)))
        for k, dt in ((1, 3.7), (2, 7.4), (3, 11.1)):
            due.append((t + dt + 1.8 * (c == 3), functools.partial(both, rs, c, k)))
    for _, event in sorted(due, key=lambda e: e[0]):
        event()

    ggt[...] = gg[...].astype(F32).T.astype(BF)
    hdt[...] = hd[...].astype(F32).T.astype(BF)

    def weight_grads(i, carry):
        out = pl.ds(pl.multiple_of(i * 256, 256), 256)
        xm = jnp.concatenate([arr[2 * i, :, 0].reshape(512, 128), arr[2 * i + 1, :, 0].reshape(512, 128)], axis=1)
        both_grads = nn(ggt[...], xm).astype(BF)
        o_wg[0, :, out] = both_grads[0:128]
        o_wu[0, :, out] = both_grads[128:256]
        xc = jnp.concatenate([arr[2 * i, :, 1].reshape(512, 128), arr[2 * i + 1, :, 1].reshape(512, 128)], axis=1)
        o_wd[0, :, out] = nn(hdt[...], xc).astype(BF)
        return carry

    lax.fori_loop(0, 8, weight_grads, 0)
    landed(ret.at[1:32, 0:CAP], ret_sem)
    mine = tn(onehot[...], ret[...].reshape(32 * SLOT, 128)).astype(BF)
    o_moe[...] = mine
    stream = (cot_v[:, col].astype(F32) + mine.astype(F32)).astype(BF)

    landed(mixall.at[1:16], w_sem.at[0])
    for i in range(4):
        pq = nn(mixall[4 * i : 4 * i + 4].reshape(256, 192), stream).astype(BF).reshape(4, 2, 32, 128)
        for h in (0, 1):
            qb[h, 4 * i : 4 * i + 4] = pq[:, h]
    push(qb.at[1 - core], qp, 21, q_sem.at[0], partner)
    landed(opt.at[1:16], w_sem.at[1])
    for i in range(4):
        pa = nt(opt[4 * i : 4 * i + 4].reshape(256, 128), stream).astype(BF)
        ab[4 * i : 4 * i + 4] = pa.reshape(4, 64, 192)
    landed(qp, q_sem.at[0])
    qs[...] = (qb[core].astype(F32) + qp[...].astype(F32)).astype(BF)
    qx[0] = qs[0]
    for lane, b in lanes():
        push(qs.at[b], qx.at[16 - b], 22, q_sem.at[3], (sp, lane))
    for lane, b in lanes():
        push(ab.at[b], ar.at[16 - b], 23, w_sem.at[2], (sp, lane))
    landed(qx.at[1:16], q_sem.at[3])
    for o in order[:0:-1]:
        zz = lax.rem(z + o + 16, 16)
        push(
            qx.at[lax.rem(zz - tp + 16, 16)], qr.at[PLACE[(-o) % 16]], 24, q_sem.at[1], (zz * 2 + core, tp)
        )
    landed(ar.at[1:16], w_sem.at[2])
    act_grad = ab[0].astype(F32)
    for b in range(1, 16):
        act_grad = act_grad + ar[b].astype(F32)

    o_gb[...] = (act_grad * conv[...]).astype(BF)
    cg[...] = jnp.zeros(cg.shape, F32)
    cg[:, 0:192] = act_grad * gb[...].astype(F32)
    cg_tile[...] = pltpu.roll(cg[:, 0:128], 64, 1)
    push(cg_tile, cg_halo, 25, hl_sem.at[1], ahead)
    landed(cg_halo, hl_sem.at[1])
    later = jnp.where(sp == 31, 0.0, cg_halo[...])
    cg[:, 128:256] = jnp.where(lane_id < 64, cg[:, 128:256], later)
    g = cg[...]
    mixed_grad = (
        taps[2] * g + taps[1] * pltpu.roll(g, 255, 1) + taps[0] * pltpu.roll(g, 254, 1)
    )[:, 0:192]
    o_gc[...] = (mixed_grad * vx[...].astype(F32)).astype(BF)
    o_vx[...] = (mixed_grad * gc[...].astype(F32)).astype(BF)

    total = qx[lax.rem(z - tp + 16, 16)].astype(F32)
    landed(qr.at[1:16], q_sem.at[1])
    for o in order[1:]:
        total = total + qr[PLACE[o % 16]].astype(F32)
    ts[...] = total
    push(ts, tp_buf, 26, q_sem.at[2], partner)
    landed(tp_buf, q_sem.at[2])
    low = jnp.where(core == 0, ts[...], tp_buf[...])
    high = jnp.where(core == 0, tp_buf[...], ts[...])
    for h, v in ((0, low), (1, high)):
        v = jnp.where(core == 0, v, pltpu.roll(v, 64, 1))
        o_proj[32 * h : 32 * h + 32, :] = v[:, 0:64]

    left(send.at[1:32, :, 0:CAP], 0)
    left(mx_tile, 1)
    for i in range(8):
        left(arr.at[0:15, 4 * i : 4 * i + 4, :, 0:CAP], 2 + i)
        left(arr.at[0:15, 4 * i : 4 * i + 4, 0, 0:CAP], 10 + i)
    left(ret.at[1:32, 0:CAP], 18)
    left(mixall.at[1:16], 19)
    left(opt.at[1:16], 20)
    left(qp, 21)
    left(qx.at[1:16], 22)
    left(ar.at[1:16], 23)
    left(qr.at[1:16], 24)
    left(cg_tile, 25)
    left(ts, 26)


def copy_kernel(*refs):
    ins, outs, sem = refs[:8], refs[8:16], refs[16]
    copies = [pltpu.make_async_copy(a, o, sem.at[i]) for i, (a, o) in enumerate(zip(ins, outs))]
    for c in copies:
        c.start()
    for c in copies:
        c.wait()


def handed_out(arrays):
    return pl.pallas_call(
        copy_kernel,
        out_shape=tuple(jax.ShapeDtypeStruct(a.shape, a.dtype) for a in arrays),
        in_specs=[pl.BlockSpec(memory_space=pltpu.VMEM)] * 8,
        out_specs=tuple([pl.BlockSpec(memory_space=pltpu.HBM)] * 8),
        scratch_shapes=[pltpu.SemaphoreType.DMA((8,))],
        compiler_params=pltpu.CompilerParams(vmem_limit_bytes=8 * 1024 * 1024),
    )(*arrays)


def on_device(
    moe_in, cotangent, routing, route_weight, w_gate, w_up, w_down, gate_b, gate_c, value_x, conv_taps, out_proj
):
    hbm = pl.BlockSpec(memory_space=pltpu.HBM)
    vmem = pl.BlockSpec(memory_space=pltpu.VMEM)
    dma = pltpu.SemaphoreType.DMA
    grads = pl.pallas_call(
        kernel,
        out_shape=(
            VM(w_gate.shape, BF), VM(w_up.shape, BF), VM(w_down.shape, BF), VM((192, 128), BF), VM((64, 64), F32),
            VM((64, 192), BF), VM((64, 192), BF), VM((64, 192), BF),
        ),
        in_specs=[hbm] * 12,
        out_specs=tuple([vmem] * 8),
        scratch_shapes=[
            VM((2, 192), jnp.int32), VM((2, 192), F32), VM((3, 64), F32), VM((128, 256), F32), VM((256, 128), F32),
            VM((192, 128), BF), VM((192, 2048), BF), VM((256, 2048), BF), VM((128, 2048), BF),
            VM((64, 192), BF), VM((64, 192), BF), VM((64, 192), BF), VM((64, 2048), BF),
            VM((512, 192), BF), VM((32, 2, SLOT, 128), BF), VM((16, 32, 2, SLOT, 128), BF),
            VM((512, 256), BF), VM((512, 128), BF), VM((4, 4, 32, SLOT, 128), BF),
            VM((8, 2, 4, 2, SLOT, 128), BF), VM((8, 2, 4, 4, SLOT, 128), BF), VM((2, 4, 4, SLOT, 128), BF), VM((8, 4, 4, SLOT, 128), BF),
            VM((8, 3, 4, SLOT, 128), BF), VM((32, SLOT, 128), BF),
            VM((32, SLOT, 128), BF),
            VM((256, 512), BF), VM((128, 512), BF),
            VM((16, 64, 192), BF), VM((16, 64, 128), BF), VM((16, 64, 192), BF), VM((16, 64, 192), BF), VM((16, 32, 128), BF),
            VM((64, 256), F32), VM((64, 128), BF), VM((64, 128), BF), VM((64, 192), F32), VM((64, 192), BF),
            VM((64, 256), F32), VM((64, 128), F32), VM((64, 128), F32),
            VM((2, 16, 32, 128), BF), VM((16, 32, 128), BF), VM((16, 32, 128), BF), VM((16, 32, 128), BF),
            VM((32, 128), F32), VM((32, 128), F32),
            dma((12,)), dma((27,)), dma((9,)), dma((8, 15)), dma((8, 7)), dma, dma((3,)), dma((2,)),
            dma((4,)),
        ],
        compiler_params=pltpu.CompilerParams(
            collective_id=0, has_side_effects=True, vmem_limit_bytes=60 * 1024 * 1024
        ),
    )(
        moe_in, cotangent, routing.T, route_weight.T, w_gate, w_up, w_down, gate_b, gate_c, value_x, conv_taps, out_proj
    )
    return handed_out(grads)


def solution(mesh):
    in_specs = (
        P("sp", None), P("sp", None), P("sp", None), P("sp", None),
        P("sp", "tp", None), P("sp", "tp", None), P("sp", "tp", None),
        P("tp", "sp"), P("tp", "sp"), P("tp", "sp"), P(None, "tp"), P("tp", None),
    )
    out_specs = (
        P("sp", "tp", None), P("sp", "tp", None), P("sp", "tp", None),
        P("sp", "tp"), P("tp", "sp"), P("tp", "sp"), P("tp", "sp"), P("tp", "sp"),
    )
    return jax.shard_map(on_device, mesh=mesh, in_specs=in_specs, out_specs=out_specs, check_vma=False)
```

```python
import functools

import jax
import jax.numpy as jnp
from jax import lax
from jax.experimental import pallas as pl
from jax.experimental.pallas import tpu as pltpu
from jax.sharding import PartitionSpec as P

MESH = pl.DeviceIdType.MESH
BF = jnp.bfloat16
F32 = jnp.float32
VM = pltpu.VMEM

OFFSETS = (0, 1, -2, 3, -4, 5, -6, 7, -1, 2, -3, 4, -5, 6, -7, 8)
PLACE = {d % 16: j for j, d in enumerate(OFFSETS)}
SLOT = 16
CAP = 12


def nt(a, b):
    return lax.dot_general(a, b, (((1,), (1,)), ((), ())), preferred_element_type=F32)


def nn(a, b):
    return jnp.dot(a, b, preferred_element_type=F32)


def tn(a, b):
    return lax.dot_general(a, b, (((0,), (0,)), ((), ())), preferred_element_type=F32)


def kernel(
    moe_h, cot_h, route_h, weight_h, wg_h, wu_h, wd_h, gb_h, gc_h, vx_h, taps_h, op_h,
    o_wg, o_wu, o_wd, o_moe, o_proj, o_gb, o_gc, o_vx,
    route_t, weight_v, taps_v, table, turned, moe_v, cot_v, wgu, wdn, gb, gc, vx, op,
    onehot, send, arr, gg, hd, part, r1, r2, r3, zb, t1, fin, ret,
    ggt, hdt, mixall, opt, ab, ar, qx,
    mixed, mx_tile, mx_halo, conv, act, cg, cg_tile, cg_halo,
    qb, qp, qs, qr, ts, tp_buf,
    in_sem, snd, z1_sem, ag_sem, rs_sem, ret_sem, w_sem, hl_sem, q_sem, tok,
):
    sp = lax.axis_index("sp")
    tp = lax.axis_index("tp")
    z, core = sp // 2, lax.rem(sp, 2)
    y, x = tp // 4, lax.rem(tp, 4)
    partner = (z * 2 + 1 - core, tp)

    def near(dim, s):
        if dim == "x":
            return (sp, y * 4 + lax.rem(x + s + 4, 4))
        return (sp, lax.rem(y + s + 4, 4) * 4 + x)

    barrier = pltpu.get_barrier_semaphore()
    order = (0, 1, -1, 2, -2, 3, -3, 4, -4, 5, -5, 6, -6, 7, -7, 8)
    for o in order[8::-1]:
        zz = lax.rem(z + o + 16, 16)
        for cc in (0, 1):
            if o == 0:
                if cc == 0:
                    pl.semaphore_signal(barrier, inc=1, device_id=partner, device_id_type=MESH)
            else:
                pl.semaphore_signal(barrier, inc=1, device_id=(zz * 2 + cc, tp), device_id_type=MESH)
    for b in range(1, 16):
        pl.semaphore_signal(barrier, inc=1, device_id=(sp, lax.rem(tp + b, 16)), device_id_type=MESH)

    small = [
        pltpu.make_async_copy(route_h, route_t, in_sem.at[9]),
        pltpu.make_async_copy(weight_h, weight_v, in_sem.at[10]),
        pltpu.make_async_copy(taps_h, taps_v, in_sem.at[11]),
    ]
    for c in small:
        c.start()
    col = pl.ds(pl.multiple_of(tp * 128, 128), 128)
    loads = [
        pltpu.make_async_copy(moe_h.at[:, col], moe_v, in_sem.at[0]),
        pltpu.make_async_copy(cot_h, cot_v, in_sem.at[1]),
        pltpu.make_async_copy(gc_h, gc, in_sem.at[2]),
        pltpu.make_async_copy(vx_h, vx, in_sem.at[3]),
        pltpu.make_async_copy(gb_h, gb, in_sem.at[4]),
        pltpu.make_async_copy(wg_h.at[0], wgu.at[0:128], in_sem.at[5]),
        pltpu.make_async_copy(wu_h.at[0], wgu.at[128:256], in_sem.at[6]),
        pltpu.make_async_copy(wd_h.at[0], wdn, in_sem.at[7]),
        pltpu.make_async_copy(op_h, op, in_sem.at[8]),
    ]
    for c in loads:
        c.start()

    def push(src, dst, group, recv, dev):
        pltpu.make_async_remote_copy(
            src_ref=src, dst_ref=dst, send_sem=snd.at[group], recv_sem=recv, device_id=dev, device_id_type=MESH
        ).start()

    def landed(ref, recv):
        pltpu.make_async_remote_copy(
            src_ref=ref, dst_ref=ref, send_sem=snd.at[0], recv_sem=recv, device_id=partner, device_id_type=MESH
        ).wait_recv()

    def left(ref, group):
        pltpu.make_async_remote_copy(
            src_ref=ref, dst_ref=ref, send_sem=snd.at[group], recv_sem=z1_sem.at[0], device_id=partner,
            device_id_type=MESH,
        ).wait_send()

    def clear(i, carry):
        arr[i, :, :, CAP:SLOT] = jnp.zeros((32, 2, SLOT - CAP, 128), BF)
        return carry

    lax.fori_loop(0, 16, clear, 0)
    ret[:, CAP:SLOT] = jnp.zeros((32, SLOT - CAP, 128), BF)

    table[...] = jnp.zeros(table.shape, F32)
    for c in small:
        c.wait()
    table[0:2, 0:192] = weight_v[...]
    table[8:11, 0:64] = taps_v[...]
    turned[...] = table[...].T
    taps = [turned[0:64, 8 + j : 9 + j] for j in range(3)]

    expert = lax.broadcasted_iota(jnp.int32, (32, 192), 0)
    first = (route_t[0:1, :] == expert).astype(F32)
    second = (route_t[1:2, :] == expert).astype(F32)
    before = (
        lax.broadcasted_iota(jnp.int32, (192, 192), 0) < lax.broadcasted_iota(jnp.int32, (192, 192), 1)
    ).astype(F32)
    rank = nn((first + second).astype(BF), before.astype(BF))
    spread = (
        (((lax.broadcasted_iota(jnp.int32, (32 * SLOT, 32), 0) >> 4) + sp) & 31)
        == lax.broadcasted_iota(jnp.int32, (32 * SLOT, 32), 1)
    ).astype(F32).astype(BF)
    place = (lax.broadcasted_iota(jnp.int32, (32 * SLOT, 192), 0) & (SLOT - 1)).astype(F32)
    hot0 = (nn(spread, jnp.where(first > 0, rank, -1.0).astype(BF)) == place).astype(F32)
    hot1 = (nn(spread, jnp.where(second > 0, rank, -1.0).astype(BF)) == place).astype(F32)
    onehot[...] = (hot0 + hot1).astype(BF)
    loads[0].wait()
    send[:, 0] = nn(onehot[...], moe_v[...]).astype(BF).reshape(32, SLOT, 128)
    loads[1].wait()
    cot_part = cot_v[:, col].astype(F32)
    cot0 = (turned[0:192, 0:1] * cot_part).astype(BF)
    cot1 = (turned[0:192, 1:2] * cot_part).astype(BF)
    routed = nn(hot0.astype(BF), cot0) + nn(hot1.astype(BF), cot1)
    send[:, 1] = routed.astype(BF).reshape(32, SLOT, 128)

    loads[2].wait()
    loads[3].wait()
    mixed[...] = jnp.zeros(mixed.shape, F32)
    mixed[:, 0:192] = (gc[...].astype(F32) * vx[...].astype(F32)).astype(BF).astype(F32)
    mx_tile[...] = pltpu.roll(mixed[:, 128:256], 64, 1).astype(BF)

    arr[tp, core, :, 0:CAP] = send[0, :, 0:CAP]
    pl.semaphore_wait(barrier, 32)

    for way, o in ((0, -4), (1, 4)):
        pl.semaphore_signal(
            tok.at[way], inc=1, device_id=(lax.rem(z + o + 16, 16) * 2 + core, tp), device_id_type=MESH
        )

    def dispatch_to(o):
        j = PLACE[(-o) % 16]
        zz = lax.rem(z + o + 16, 16)
        for cc in (0, 1):
            e = zz * 2 + cc
            if o == 0:
                if cc == 1:
                    continue
                e = z * 2 + 1 - core
            push(
                send.at[lax.rem(e - sp + 32, 32), :, 0:CAP], arr.at[tp, j * 2 + core, :, 0:CAP], 0,
                z1_sem.at[8 if o == 0 else j // 2], (e, tp),
            )

    def dispatch(*chunks):
        for o in order:
            if PLACE[(-o) % 16] % 8 // 2 in chunks:
                dispatch_to(o)

    dispatch(0, 1)
    after = (lax.rem(sp + 1, 32), tp)
    ahead = (lax.rem(sp + 31, 32), tp)
    push(mx_tile, mx_halo, 1, hl_sem.at[0], after)

    def z_arrived(i):
        a = 4 * i
        if i == 0:
            landed(arr.at[tp, 1 - core, :, 0:CAP], z1_sem.at[8])
            a = 2
        landed(arr.at[tp, a : 4 * i + 4, :, 0:CAP], z1_sem.at[i])

    def gather_steps(region, dims, group, sem, direct):
        d1, d2 = dims

        def lane(a, b):
            dx, dy = (a, b) if d1 == "x" else (b, a)
            return lax.rem(y + dy + 4, 4) * 4 + lax.rem(x + dx + 4, 4)

        def half(s):
            return 0 if s == 1 else 1

        ids = {0: 0, 1: 1, -1: 2, 2: 3}

        def sem1(s):
            return sem(0 if s == 1 else 1)

        def sem2(i, s):
            return sem(3 + ids[i] * 3 + (0 if s == 1 else 1))

        def sem2f(i):
            return sem(3 + ids[i] * 3 + 2)

        def e0():
            own = region(lane(0, 0))
            for s in (1, -1):
                push(own, own, group, sem1(s), near(d1, s))
            if direct:
                push(own, own, group, sem(2), near(d1, 2))
            for s in (1, -1):
                push(own, own, group, sem2(0, s), near(d2, s))

        def across(i):
            block = region(lane(i, 0))
            for s in (1, -1):
                push(block, block, group, sem2(i, s), near(d2, s))

        def on(i):
            for s in (1, -1):
                landed(region(lane(i, -s)), sem2(i, s))
                block = region(lane(i, -s), half(s))
                push(block, block, group, sem2f(i), near(d2, s))

        def e1():
            for s in (1, -1):
                landed(region(lane(-s, 0)), sem1(s))
                if not direct:
                    block = region(lane(-s, 0), half(s))
                    push(block, block, group, sem(2), near(d1, s))
            for s in (1, -1):
                across(-s)
            on(0)

        def e2():
            landed(region(lane(2, 0)), sem(2))
            across(2)

        def e3():
            on(1)
            on(-1)
            on(2)

        def e4():
            for i in (0, 1, -1, 2):
                landed(region(lane(i, 2)), sem2f(i))

        return e0, e1, e2, e3, e4

    def rows_of(q):
        def region(lane, h=None):
            a, n = (4 * q, 4) if h is None else (4 * q + 2 * h, 2)
            return arr.at[lane, a : a + n, :, 0:CAP]

        return region

    dims_of = (("x", "y"), ("x", "y"), ("y", "x"), ("y", "x"))
    ag = [
        gather_steps(rows_of(i), dims_of[i // 2], 2 + i, functools.partial(lambda i, k: ag_sem.at[i, k], i), True)
        for i in range(8)
    ]

    def expert_rows(c):
        parts = (4 * c, 4 * c + 16)

        def wide(kind):
            return jnp.concatenate(
                [
                    jnp.concatenate([arr[l, a : a + 4, kind].reshape(64, 128) for a in parts], axis=0)
                    for l in range(16)
                ],
                axis=1,
            )

        pre = nt(wide(0), wgu[...])
        hg = nt(wide(1), wdn[...])
        gate, up = pre[:, 0:128], pre[:, 128:256]
        sig = jax.nn.sigmoid(gate)
        silu = gate * sig
        hidden = (silu * up).astype(BF)
        g = jnp.concatenate([hg * up * sig * (1.0 + gate * (1.0 - sig)), hg * silu], axis=1).astype(BF)
        for h, a in enumerate(parts):
            hd[16 * a : 16 * a + 64, :] = hidden[64 * h : 64 * h + 64]
            gg[16 * a : 16 * a + 64, :] = g[64 * h : 64 * h + 64]
        for i in range(8):
            pv = nn(g, wgu[:, 256 * i : 256 * i + 256]).astype(BF)
            for k in (0, 1):
                l = 2 * i + k
                for h, a in enumerate(parts):
                    part[l // 4, l % 4, a : a + 4] = pv[
                        64 * h : 64 * h + 64, 128 * k : 128 * k + 128
                    ].reshape(4, SLOT, 128)

    def back(owner):
        return lax.rem(sp - owner + 32, 32)

    def scatter_steps(q, dims):
        d1, d2 = dims
        at = {"x": x, "y": y}
        a = 4 * q

        def half(s):
            return (0, 2) if s == 1 else (2, 2)

        def bundle(d, lo=0, n=4):
            i = lax.rem(at[d1] + d + 4, 4)
            if d1 == "y":
                return part.at[i, :, a + lo : a + lo + n]
            return part.at[:, i, a + lo : a + lo + n]

        def cut(ref, dims=4):
            return ref.at[:, :, 0:CAP] if dims == 4 else ref.at[:, 0:CAP]

        def w(s):
            return 0 if s == 1 else 1

        def sem(i):
            return rs_sem.at[q, i]

        direct = q % 4 == 3

        def q1():
            if direct:
                push(cut(bundle(2)), cut(r3.at[q // 4]), 10 + q, sem(0), near(d1, 2))
                for s in (1, -1):
                    push(cut(bundle(s)), cut(r2.at[q, w(s)]), 10 + q, sem(2 + w(s)), near(d1, s))
                return
            for s in (1, -1):
                push(cut(bundle(2, *half(s))), cut(r1.at[q, w(s)]), 10 + q, sem(w(s)), near(d1, s))

        def q2():
            if direct:
                return
            for s in (1, -1):
                landed(cut(r1.at[q, w(s)]), sem(w(s)))
                mine = bundle(s, *half(s))
                mine[...] = (mine[...].astype(F32) + r1[q, w(s)].astype(F32)).astype(BF)
                push(cut(bundle(s)), cut(r2.at[q, w(s)]), 10 + q, sem(2 + w(s)), near(d1, s))

        def q3():
            for s in (1, -1):
                landed(cut(r2.at[q, w(s)]), sem(2 + w(s)))
            own = bundle(0)[...].astype(F32)
            if direct:
                landed(cut(r3.at[q // 4]), sem(0))
                own = own + r3[q // 4].astype(F32)
            zb[q] = (own + r2[q, 0].astype(F32) + r2[q, 1].astype(F32)).astype(BF)
            for k, s in enumerate((2, 1, -1)):
                i = lax.rem(at[d2] + s + 4, 4)
                push(cut(zb.at[q, i], 3), cut(t1.at[q, k], 3), 10 + q, sem(4 + k), near(d2, s))

        def q4():
            for k in range(3):
                landed(cut(t1.at[q, k], 3), sem(4 + k))
            fin[a : a + 4] = (
                zb[q, at[d2]].astype(F32) + t1[q, 0].astype(F32) + t1[q, 1].astype(F32) + t1[q, 2].astype(F32)
            ).astype(BF)
            for j in (2 * q + 1, 2 * q):
                for cc in (0, 1):
                    if OFFSETS[j] == 0:
                        if cc == 0:
                            push(fin.at[1 - core, 0:CAP], ret.at[back(partner[0]), 0:CAP], 18, ret_sem, partner)
                            ret[0, 0:CAP] = fin[core, 0:CAP]
                    else:
                        dev = (lax.rem(z + OFFSETS[j] + 16, 16) * 2 + cc, tp)
                        push(fin.at[2 * j + cc, 0:CAP], ret.at[back(dev[0]), 0:CAP], 18, ret_sem, dev)

        return q1, q2, q3, q4

    rs = [scatter_steps(i, dims_of[i // 2][::-1]) for i in range(8)]

    def both(steps, c, k):
        steps[c][k]()
        steps[c + len(steps) // 2][k]()

    lane_id = lax.broadcasted_iota(jnp.int32, (64, 128), 1)

    def start(i):
        z_arrived(i)
        ag[i][0]()
        if i == 0:
            for way in (0, 1):
                pl.semaphore_wait(tok.at[way], 1)
            dispatch(2, 3)

    def step(steps, i, k):
        steps[i][k]()

    def forward():
        loads[4].wait()
        landed(mx_halo, hl_sem.at[0])
        halo = jnp.where(sp == 0, 0.0, mx_halo[...].astype(F32))
        mixed[:, 128:256] = jnp.where(lane_id < 64, mixed[:, 128:256], halo)
        m = mixed[...]
        conv[...] = (
            taps[2] * m + taps[1] * pltpu.roll(m, 1, 1) + taps[0] * pltpu.roll(m, 2, 1)
        )[:, 0:192]
        act[...] = (gb[...].astype(F32) * conv[...]).astype(BF)
        for c in loads[5:9]:
            c.wait()

    def rows(c):
        both(ag, c, 4)
        expert_rows(c)
        both(rs, c, 0)

    plane = sorted(
        ((dy, dx) for dy in range(4) for dx in range(4) if (dy, dx) != (0, 0)),
        key=lambda d: -(min(d[0], 4 - d[0]) + min(d[1], 4 - d[1])),
    )

    def lanes():
        for dy, dx in plane:
            lane = lax.rem(y + dy, 4) * 4 + lax.rem(x + dx, 4)
            yield lane, lax.rem(lane - tp + 16, 16)

    def exchange():
        mixall[0] = act[...]
        opt[0] = op[:, col]
        for lane, b in lanes():
            push(act, mixall.at[16 - b], 19, w_sem.at[0], (sp, lane))
        for lane, b in lanes():
            there = pl.ds(pl.multiple_of(lane * 128, 128), 128)
            push(op.at[:, there], opt.at[16 - b], 20, w_sem.at[1], (sp, lane))

    due = [(17.3, forward), (46.0, exchange)]
    for i, t in enumerate((10.7, 13.5, 16.5, 20.0, 12.0, 15.0, 17.5, 20.8)):
        due.append((t, functools.partial(start, i)))
        for k, dt in ((1, 4.2), (2, 4.8), (3, 9.0)):
            due.append((t + dt, functools.partial(step, ag, i, k)))
    for c, t in enumerate((26.5, 29.5, 32.0, 33.5)):
        due.append((t, functools.partial(rows, c)))
        last = 43.0 + 0.2 * c if c < 3 else 46.4
        for k, u in ((1, t + 3.7), (2, 42.7 if c == 3 else t + 7.4), (3, last)):
            due.append((u, functools.partial(both, rs, c, k)))
    for _, event in sorted(due, key=lambda e: e[0]):
        event()

    ggt[...] = gg[...].astype(F32).T.astype(BF)
    hdt[...] = hd[...].astype(F32).T.astype(BF)

    def weight_grads(i, carry):
        out = pl.ds(pl.multiple_of(i * 256, 256), 256)
        xm = jnp.concatenate([arr[2 * i, :, 0].reshape(512, 128), arr[2 * i + 1, :, 0].reshape(512, 128)], axis=1)
        both_grads = nn(ggt[...], xm).astype(BF)
        o_wg[0, :, out] = both_grads[0:128]
        o_wu[0, :, out] = both_grads[128:256]
        xc = jnp.concatenate([arr[2 * i, :, 1].reshape(512, 128), arr[2 * i + 1, :, 1].reshape(512, 128)], axis=1)
        o_wd[0, :, out] = nn(hdt[...], xc).astype(BF)
        return carry

    lax.fori_loop(0, 8, weight_grads, 0)
    landed(ret.at[1:32, 0:CAP], ret_sem)
    mine = tn(onehot[...], ret[...].reshape(32 * SLOT, 128)).astype(BF)
    o_moe[...] = mine
    stream = (cot_v[:, col].astype(F32) + mine.astype(F32)).astype(BF)

    landed(mixall.at[1:16], w_sem.at[0])
    for i in range(4):
        pq = nn(mixall[4 * i : 4 * i + 4].reshape(256, 192), stream).astype(BF).reshape(4, 2, 32, 128)
        for h in (0, 1):
            qb[h, 4 * i : 4 * i + 4] = pq[:, h]
    push(qb.at[1 - core], qp, 21, q_sem.at[0], partner)
    landed(opt.at[1:16], w_sem.at[1])
    for i in range(4):
        pa = nt(opt[4 * i : 4 * i + 4].reshape(256, 128), stream).astype(BF)
        ab[4 * i : 4 * i + 4] = pa.reshape(4, 64, 192)
    landed(qp, q_sem.at[0])
    qs[...] = (qb[core].astype(F32) + qp[...].astype(F32)).astype(BF)
    qx[0] = qs[0]
    for lane, b in lanes():
        push(qs.at[b], qx.at[16 - b], 22, q_sem.at[3], (sp, lane))
    for lane, b in lanes():
        push(ab.at[b], ar.at[16 - b], 23, w_sem.at[2], (sp, lane))
    landed(qx.at[1:16], q_sem.at[3])
    for o in order[:0:-1]:
        zz = lax.rem(z + o + 16, 16)
        push(
            qx.at[lax.rem(zz - tp + 16, 16)], qr.at[PLACE[(-o) % 16]], 24, q_sem.at[1], (zz * 2 + core, tp)
        )
    landed(ar.at[1:16], w_sem.at[2])
    act_grad = ab[0].astype(F32)
    for b in range(1, 16):
        act_grad = act_grad + ar[b].astype(F32)

    o_gb[...] = (act_grad * conv[...]).astype(BF)
    cg[...] = jnp.zeros(cg.shape, F32)
    cg[:, 0:192] = act_grad * gb[...].astype(F32)
    cg_tile[...] = pltpu.roll(cg[:, 0:128], 64, 1)
    push(cg_tile, cg_halo, 25, hl_sem.at[1], ahead)
    landed(cg_halo, hl_sem.at[1])
    later = jnp.where(sp == 31, 0.0, cg_halo[...])
    cg[:, 128:256] = jnp.where(lane_id < 64, cg[:, 128:256], later)
    g = cg[...]
    mixed_grad = (
        taps[2] * g + taps[1] * pltpu.roll(g, 255, 1) + taps[0] * pltpu.roll(g, 254, 1)
    )[:, 0:192]
    o_gc[...] = (mixed_grad * vx[...].astype(F32)).astype(BF)
    o_vx[...] = (mixed_grad * gc[...].astype(F32)).astype(BF)

    total = qx[lax.rem(z - tp + 16, 16)].astype(F32)
    landed(qr.at[1:16], q_sem.at[1])
    for o in order[1:]:
        total = total + qr[PLACE[o % 16]].astype(F32)
    ts[...] = total
    push(ts, tp_buf, 26, q_sem.at[2], partner)
    landed(tp_buf, q_sem.at[2])
    low = jnp.where(core == 0, ts[...], tp_buf[...])
    high = jnp.where(core == 0, tp_buf[...], ts[...])
    for h, v in ((0, low), (1, high)):
        v = jnp.where(core == 0, v, pltpu.roll(v, 64, 1))
        o_proj[32 * h : 32 * h + 32, :] = v[:, 0:64]

    left(send.at[1:32, :, 0:CAP], 0)
    left(mx_tile, 1)
    for i in range(8):
        left(arr.at[0:15, 4 * i : 4 * i + 4, :, 0:CAP], 2 + i)
        left(arr.at[0:15, 4 * i : 4 * i + 4, 0, 0:CAP], 10 + i)
    left(ret.at[1:32, 0:CAP], 18)
    left(mixall.at[1:16], 19)
    left(opt.at[1:16], 20)
    left(qp, 21)
    left(qx.at[1:16], 22)
    left(ar.at[1:16], 23)
    left(qr.at[1:16], 24)
    left(cg_tile, 25)
    left(ts, 26)


def copy_kernel(*refs):
    ins, outs, sem = refs[:8], refs[8:16], refs[16]
    copies = [pltpu.make_async_copy(a, o, sem.at[i]) for i, (a, o) in enumerate(zip(ins, outs))]
    for c in copies:
        c.start()
    for c in copies:
        c.wait()


def handed_out(arrays):
    return pl.pallas_call(
        copy_kernel,
        out_shape=tuple(jax.ShapeDtypeStruct(a.shape, a.dtype) for a in arrays),
        in_specs=[pl.BlockSpec(memory_space=pltpu.VMEM)] * 8,
        out_specs=tuple([pl.BlockSpec(memory_space=pltpu.HBM)] * 8),
        scratch_shapes=[pltpu.SemaphoreType.DMA((8,))],
        compiler_params=pltpu.CompilerParams(vmem_limit_bytes=8 * 1024 * 1024),
    )(*arrays)


def on_device(
    moe_in, cotangent, routing, route_weight, w_gate, w_up, w_down, gate_b, gate_c, value_x, conv_taps, out_proj
):
    hbm = pl.BlockSpec(memory_space=pltpu.HBM)
    vmem = pl.BlockSpec(memory_space=pltpu.VMEM)
    dma = pltpu.SemaphoreType.DMA
    grads = pl.pallas_call(
        kernel,
        out_shape=(
            VM(w_gate.shape, BF), VM(w_up.shape, BF), VM(w_down.shape, BF), VM((192, 128), BF), VM((64, 64), F32),
            VM((64, 192), BF), VM((64, 192), BF), VM((64, 192), BF),
        ),
        in_specs=[hbm] * 12,
        out_specs=tuple([vmem] * 8),
        scratch_shapes=[
            VM((2, 192), jnp.int32), VM((2, 192), F32), VM((3, 64), F32), VM((128, 256), F32), VM((256, 128), F32),
            VM((192, 128), BF), VM((192, 2048), BF), VM((256, 2048), BF), VM((128, 2048), BF),
            VM((64, 192), BF), VM((64, 192), BF), VM((64, 192), BF), VM((64, 2048), BF),
            VM((512, 192), BF), VM((32, 2, SLOT, 128), BF), VM((16, 32, 2, SLOT, 128), BF),
            VM((512, 256), BF), VM((512, 128), BF), VM((4, 4, 32, SLOT, 128), BF),
            VM((8, 2, 4, 2, SLOT, 128), BF), VM((8, 2, 4, 4, SLOT, 128), BF), VM((2, 4, 4, SLOT, 128), BF), VM((8, 4, 4, SLOT, 128), BF),
            VM((8, 3, 4, SLOT, 128), BF), VM((32, SLOT, 128), BF),
            VM((32, SLOT, 128), BF),
            VM((256, 512), BF), VM((128, 512), BF),
            VM((16, 64, 192), BF), VM((16, 64, 128), BF), VM((16, 64, 192), BF), VM((16, 64, 192), BF), VM((16, 32, 128), BF),
            VM((64, 256), F32), VM((64, 128), BF), VM((64, 128), BF), VM((64, 192), F32), VM((64, 192), BF),
            VM((64, 256), F32), VM((64, 128), F32), VM((64, 128), F32),
            VM((2, 16, 32, 128), BF), VM((16, 32, 128), BF), VM((16, 32, 128), BF), VM((16, 32, 128), BF),
            VM((32, 128), F32), VM((32, 128), F32),
            dma((12,)), dma((27,)), dma((9,)), dma((8, 15)), dma((8, 7)), dma, dma((3,)), dma((2,)),
            dma((4,)), pltpu.SemaphoreType.REGULAR((2,)),
        ],
        compiler_params=pltpu.CompilerParams(
            collective_id=0, has_side_effects=True, vmem_limit_bytes=60 * 1024 * 1024
        ),
    )(
        moe_in, cotangent, routing.T, route_weight.T, w_gate, w_up, w_down, gate_b, gate_c, value_x, conv_taps, out_proj
    )
    return handed_out(grads)


def solution(mesh):
    in_specs = (
        P("sp", None), P("sp", None), P("sp", None), P("sp", None),
        P("sp", "tp", None), P("sp", "tp", None), P("sp", "tp", None),
        P("tp", "sp"), P("tp", "sp"), P("tp", "sp"), P(None, "tp"), P("tp", None),
    )
    out_specs = (
        P("sp", "tp", None), P("sp", "tp", None), P("sp", "tp", None),
        P("sp", "tp"), P("tp", "sp"), P("tp", "sp"), P("tp", "sp"), P("tp", "sp"),
    )
    return jax.shard_map(on_device, mesh=mesh, in_specs=in_specs, out_specs=out_specs, check_vma=False)
```
